512 devices in a mesh: ra: 64 (over z, y), cb: 4 (over x), dp: 2 (over core).
Axes of the slice: x: 4, y: 8, z: 8, core: 2. Of those that a mesh axis runs over, the one named last changes fastest.
Arguments:
- tokens: bfloat16 [2048, 4096], P('dp', 'cb'), may hold values from -3000 to 3000
- norm_gain: float32 [4096], P('cb'), may hold values from 0.1 to 1.9
- norm_bias: float32 [4096], P('cb'), may hold values from -2 to 2
- gate_weight: float32 [4096, 11264], P('cb', 'ra'), may hold values from -0.09375 to 0.09375
- up_weight: float32 [4096, 11264], P('cb', 'ra'), may hold values from -0.09375 to 0.09375
- gate_scale: float32 [11264], P('ra'), may hold values from 0.5 to 2
- up_scale: float32 [11264], P('ra'), may hold values from 0.5 to 2
- down_weight: float32 [11264, 4096], P('ra', 'cb'), may hold values from -0.0546875 to 0.0546875
- down_scale: float32 [4096], P('cb'), may hold values from 0.5 to 8
- out_gain: float32 [4096], P('cb'), may hold values from 0.1 to 1.9
- out_bias: float32 [4096], P('cb'), may hold values from -2 to 2
Outputs:
- result: bfloat16 [2048, 4096], P(('dp', 'ra'), 'cb')
The draws below stay inside these ranges and needn't reach their ends.
All inputs are finite; a program needn't handle non-finite values.
Results may differ from the reference program's by a relative error of at most 0.018.
Values may be sent and summed in bfloat16 or wider, within the bound.
No kernel may reach another device: no remote copies, remote signals or barrier semaphores. Data moves between devices by JAX's collectives and lax.ppermute only.
A program may use at most 64 MiB of HBM per device.

```python
import math
import jax
import jax.numpy as jnp
from jax import lax

D = 4096
FF = 11264
TOKENS = 2048


def draw_tokens(key, part):
    keys = jax.random.split(key, 3)
    base = jax.random.normal(keys[0], (TOKENS, D), jnp.float32)
    columns = jnp.exp(math.log(6.0) * jnp.arange(D, dtype=jnp.float32) / D)
    columns = columns * jnp.exp(jax.random.uniform(keys[1], (D,), jnp.float32, -0.35, 0.35))
    rows_scale = jnp.exp(jax.random.uniform(keys[2], (TOKENS, 1), jnp.float32, 0.0, math.log(10.0)))
    values = base * columns * rows_scale
    return values.astype(jnp.bfloat16)


def draw_down_scale(key, part):
    rising = jnp.exp(math.log(4.0) * jnp.arange(D, dtype=jnp.float32) / D)
    factor = jnp.exp(jax.random.uniform(key, (D,), jnp.float32, math.log(0.5), math.log(2.0)))
    return (rising * factor).astype(jnp.float32)


def level_of(own_key, extent, pieces, smallest, high):
    def one(dim, shards_of):
        heights = jax.random.uniform(jax.random.fold_in(jax.random.fold_in(own_key, 6), dim), (shards_of,), jnp.float32, smallest / len(pieces), high / len(pieces))
        return jnp.repeat(jnp.exp(heights), extent[dim] // shards_of).reshape((-1,) + (1,) * (len(extent) - dim - 1))

    gain = one(*pieces[0])
    for cut in pieces[1:]:
        gain = gain * one(*cut)
    return gain


def gaussian(stream_key, dims, deviation, limit, pieces=(), kind=jnp.bfloat16):
    result = jax.random.normal(stream_key, dims, jnp.float32) * deviation
    if len(pieces) > 0:
        result = level_of(stream_key, dims, pieces, -0.22, 0.18) * result
    return jnp.clip(result, min=-limit, max=limit).astype(kind)


def setup_inputs(seed: int = 0) -> dict:
    streams_of = jax.random.split(jax.random.key(seed), 12)
    tokens = draw_tokens(jax.random.fold_in(streams_of[11], 71), 0)
    norm_gain = jnp.clip(1.0 + 0.18 * jax.random.normal(streams_of[1], (D,), jnp.float32), 0.1, 1.9)
    norm_bias = gaussian(streams_of[2], (D,), 0.3, 2.0, ((0, 4),), jnp.float32)
    gate_weight = gaussian(streams_of[3], (D, FF), D ** -0.5, 0.09375, ((0, 4), (1, 64)), jnp.float32)
    up_weight = gaussian(streams_of[4], (D, FF), D ** -0.5, 0.09375, ((0, 4), (1, 64)), jnp.float32)
    gate_scale = jnp.clip(jnp.exp(math.log(2.0) - 1.3862944 * jax.random.uniform(streams_of[5], (FF,), jnp.float32) ** level_of(streams_of[5], (FF,), ((0, 64),), -0.2, 0.2)), 0.5, 2.0)
    up_scale = jnp.clip(jnp.exp(math.log(2.0) - 1.3862944 * jax.random.uniform(streams_of[6], (FF,), jnp.float32) ** level_of(streams_of[6], (FF,), ((0, 64),), -0.2, 0.2)), 0.5, 2.0)
    down_weight = gaussian(streams_of[7], (FF, D), FF ** -0.5, 0.0546875, ((0, 64), (1, 4)), jnp.float32)
    down_scale = draw_down_scale(jax.random.fold_in(streams_of[11], 71), 0)
    out_gain = jnp.clip(1.0 + 0.18 * jax.random.normal(streams_of[9], (D,), jnp.float32), 0.1, 1.9)
    out_bias = gaussian(streams_of[10], (D,), 0.3, 2.0, ((0, 4),), jnp.float32)
    return dict(tokens=tokens, norm_gain=norm_gain, norm_bias=norm_bias, gate_weight=gate_weight, up_weight=up_weight, gate_scale=gate_scale, up_scale=up_scale, down_weight=down_weight, down_scale=down_scale, out_gain=out_gain, out_bias=out_bias)


def standardize(values):
    mean = lax.optimization_barrier(jnp.mean(values, axis=1, keepdims=True))
    centred = values - mean
    spread = lax.optimization_barrier(jnp.mean(centred * centred, axis=1, keepdims=True))
    return centred * lax.rsqrt(spread + 1e-05)

def reference(tokens, norm_gain, norm_bias, gate_weight, up_weight, gate_scale, up_scale, down_weight, down_scale, out_gain, out_bias):
    normed = (standardize(tokens.astype(jnp.float32)) * norm_gain + norm_bias).astype(jnp.bfloat16)
    gate = jnp.dot(normed, gate_weight.astype(jnp.bfloat16), preferred_element_type=jnp.float32) * gate_scale
    up = jnp.dot(normed, up_weight.astype(jnp.bfloat16), preferred_element_type=jnp.float32) * up_scale
    hidden = (jax.nn.silu(gate) * up).astype(jnp.bfloat16)
    branch = jnp.dot(hidden, down_weight.astype(jnp.bfloat16), preferred_element_type=jnp.float32) * down_scale
    mixed = 0.5 * normed.astype(jnp.float32) + branch
    return (standardize(mixed) * out_gain + out_bias).astype(jnp.bfloat16)
```

```python
import jax
import jax.numpy as jnp
from jax import lax
from jax.experimental import pallas as pl
from jax.experimental.pallas import tpu as pltpu
from jax.sharding import Mesh, PartitionSpec as P

D = 4096
F32 = jnp.float32
BF16 = jnp.bfloat16
RA = ("Z", "zl", "Y", "yl")
UNITS = 44
SLOT = 48
PART = 2 * SLOT
ROWS = 1024
COLS = 1024
FFL = 176
CHUNK = 256


def iota(shape, dim):
    return lax.broadcasted_iota(jnp.int32, shape, dim)


def dot(a, b, ca, cb):
    return lax.dot_general(a, b, (((ca,), (cb,)), ((), ())), preferred_element_type=F32)


def rounded(v):
    return v.astype(BF16).astype(F32)


def one_hot(cond):
    return jnp.where(cond, 1.0, 0.0).astype(BF16)


def project_kernel(x_ref, gw_ref, uw_ref, gain_ref, bias_ref, out_ref, w_ref, vec_ref):
    step = pl.program_id(0)

    @pl.when(step == 0)
    def _():
        gw = gw_ref[...].astype(BF16)
        uw = uw_ref[...].astype(BF16)
        row = iota((PART, FFL), 0)
        col = iota((PART, FFL), 1)
        for k in range(4):
            unit = col - UNITS * k
            as_gate = one_hot((unit == row) & (row < UNITS))
            as_up = one_hot((unit == row - SLOT) & (row >= SLOT) & (row < SLOT + UNITS))
            w = dot(as_gate, gw, 1, 0) + dot(as_up, uw, 1, 0)
            w_ref[PART * k : PART * (k + 1), :] = w.astype(BF16)
        gain = gain_ref[...]
        bias = bias_ref[...]
        r = iota((8, COLS), 0)
        gh = rounded(gain)
        bh = rounded(bias)
        lead = jnp.where(r == 0, gh, jnp.where(r == 1, gain - gh, jnp.where(r == 2, bh, jnp.where(r == 3, bias - bh, 0.0))))
        sums = dot(lead.astype(BF16), w_ref[...], 1, 1)
        both = jnp.concatenate(
            [sums[0:1] + sums[1:2], sums[2:3] + sums[3:4], jnp.zeros((1, ROWS - 8 * PART), F32)], axis=1
        )
        hi = rounded(both)
        q = iota((8, ROWS), 0)
        vec_ref[...] = jnp.where(q == 0, hi, jnp.where(q == 1, both - hi, 0.0))

    x = x_ref[...].reshape(CHUNK, COLS).astype(F32)
    m = jnp.sum(x, axis=1, keepdims=True) * (1.0 / COLS)
    xc = x - m
    m2 = jnp.sum(xc * xc, axis=1, keepdims=True)
    xn = (xc * gain_ref[...]).astype(BF16)
    part = dot(w_ref[...], xn, 1, 1)
    lane = iota((CHUNK, 128), 1)
    stat = jnp.where(lane == 0, m, jnp.where(lane == 1, m2, 0.0)).T
    m_row = stat[0:1]
    m2_row = stat[1:2]
    m_hi = rounded(m_row)
    m_mid = rounded(m_row - m_hi)
    m_lo = m_row - m_hi - m_mid
    m2_hi = rounded(m2_row)
    m2_lo = m2_row - m2_hi
    vec = vec_ref[:, pl.ds(pl.multiple_of(step * CHUNK, CHUNK), CHUNK)]
    r = iota((8, CHUNK), 0)
    t1 = jnp.where(r == 4, m_hi, jnp.where(r == 5, m_mid, jnp.where(r == 6, m_lo, jnp.where(r == 7, vec[0:1], 0.0))))
    t2 = jnp.where(r == 4, m2_hi, jnp.where(r == 5, m2_lo, jnp.where(r == 6, vec[1:2], 0.0)))
    z = jnp.zeros((SLOT - 8, CHUNK), F32)
    extra = jnp.concatenate([z, t1, z, t2], axis=0)
    for k in range(4):
        out_ref[k] = (part[PART * k : PART * (k + 1)] + extra).astype(BF16)


def project(tokens, gate_t, up_t, gain, bias):
    x = tokens.reshape(4, 2, 4, 2, 16, COLS)
    return pl.pallas_call(
        project_kernel,
        grid=(4,),
        in_specs=[
            pl.BlockSpec((4, 1, 4, 1, 16, COLS), lambda j: (0, j // 2, 0, j % 2, 0, 0)),
            pl.BlockSpec((FFL, COLS), lambda j: (0, 0)),
            pl.BlockSpec((FFL, COLS), lambda j: (0, 0)),
            pl.BlockSpec((1, COLS), lambda j: (0, 0)),
            pl.BlockSpec((1, COLS), lambda j: (0, 0)),
        ],
        out_specs=pl.BlockSpec((4, PART, CHUNK), lambda j: (0, 0, j)),
        out_shape=jax.ShapeDtypeStruct((4, PART, ROWS), BF16),
        scratch_shapes=[pltpu.VMEM((4 * PART, COLS), BF16), pltpu.VMEM((8, ROWS), F32)],
        compiler_params=pltpu.CompilerParams(dimension_semantics=("arbitrary",)),
        name="project",
    )(x, gate_t, up_t, gain, bias)


def hidden_kernel(idx_ref, r_ref, gs_ref, us_ref, out_ref, stat_ref):
    me = idx_ref[0]
    means = []
    m2s = []
    for c in range(4):
        a = r_ref[c, 32:48, :].astype(F32)
        b = r_ref[c, 80:96, :].astype(F32)
        means.append(a[12:13] + a[13:14] + a[14:15])
        m2s.append(b[12:13] + b[13:14])
    mean = (means[0] + means[1] + means[2] + means[3]) * 0.25
    deltas = [v - mean for v in means]
    m2 = sum(m2s) + COLS * sum(d * d for d in deltas)
    rstd = lax.rsqrt(m2 * (1.0 / D) + 1e-05)
    q = iota((8, ROWS), 0)
    stat_ref[...] = jnp.where(q == 0, mean, jnp.where(q == 1, rstd, 0.0))

    wide = 8 * PART
    pick_row = iota((2 * PART, wide), 0)
    pick_lane = iota((2 * PART, wide), 1)
    base = jnp.where(pick_row < PART, me * PART, (4 + me) * PART - PART)
    pick = one_hot(pick_lane == pick_row + base)
    tiles = [r_ref[c, 32:48, 0:wide] for c in range(4)] + [r_ref[c, 80:96, 0:wide] for c in range(4)]
    vecs = dot(pick, jnp.concatenate(tiles, axis=0), 1, 1)
    col_sums = [vecs[0:PART, 16 * c + 15 : 16 * c + 16] + vecs[0:PART, 78 + 16 * c : 79 + 16 * c] for c in range(4)]
    biases = sum(vecs[PART:, 16 * c + 15 : 16 * c + 16] + vecs[PART:, 78 + 16 * c : 79 + 16 * c] for c in range(4))

    gs = gs_ref[...]
    us = us_ref[...]
    g1 = rounded(gs)
    g2 = rounded(gs - g1)
    u1 = rounded(us)
    u2 = rounded(us - u1)
    sr = iota((16, FFL), 0)
    pieces = jnp.where(sr == 0, g1, jnp.where(sr == 1, g2, jnp.where(sr == 2, gs - g1 - g2, 0.0)))
    pieces = pieces + jnp.where(sr == 3, u1, jnp.where(sr == 4, u2, jnp.where(sr == 5, us - u1 - u2, 0.0)))
    row = iota((PART, FFL), 0)
    unit = jnp.where(row < SLOT, row, row - SLOT)
    own = one_hot((iota((PART, FFL), 1) == unit + me * UNITS) & (unit < UNITS))
    sc = dot(own, pieces.astype(BF16), 1, 1)
    scale = jnp.where(iota((PART, 1), 0) < SLOT, sc[:, 0:1] + sc[:, 1:2] + sc[:, 2:3], sc[:, 3:4] + sc[:, 4:5] + sc[:, 5:6])

    keep = iota((SLOT, CHUNK), 0) < UNITS
    for j in range(4):
        at = slice(CHUNK * j, CHUNK * (j + 1))
        acc = jnp.zeros((PART, CHUNK), F32)
        for c in range(4):
            acc = acc + (r_ref[c, :, at].astype(F32) + col_sums[c] * deltas[c][:, at])
        y = (acc * rstd[:, at] + biases) * scale
        gate = y[0:SLOT]
        up = y[SLOT:PART]
        h = jnp.where(keep, gate / (1.0 + jnp.exp(-gate)) * up, 0.0).astype(BF16)
        for k in range(4):
            out_ref[j, k] = h


def hidden_of(idx, received, gate_scale, up_scale):
    vm = pl.BlockSpec(memory_space=pltpu.VMEM)
    return pl.pallas_call(
        hidden_kernel,
        in_specs=[pl.BlockSpec(memory_space=pltpu.SMEM), vm, vm, vm],
        out_specs=[vm, vm],
        out_shape=[jax.ShapeDtypeStruct((4, 4, SLOT, CHUNK), BF16), jax.ShapeDtypeStruct((8, ROWS), F32)],
        name="hidden",
    )(idx, received, gate_scale, up_scale)


def down_kernel(idx_ref, h_ref, w0_ref, w1_ref, w2_ref, w3_ref, out_ref):
    me = idx_ref[1]
    row = iota((FFL, 4 * SLOT), 0)
    lane = iota((FFL, 4 * SLOT), 1)
    hit = lane < 0
    for k in range(4):
        hit = hit | ((lane == row + (SLOT - UNITS) * k) & (row >= UNITS * k) & (row < UNITS * (k + 1)))
    squeeze = one_hot(hit)
    acc = jnp.zeros((CHUNK, COLS), F32)
    for r, w_ref in enumerate((w0_ref, w1_ref, w2_ref, w3_ref)):
        h = dot(h_ref[me ^ r], squeeze, 0, 1).astype(BF16)
        acc = acc + dot(h, w_ref[...], 1, 0)
    out_ref[...] = acc.astype(BF16)


def down(idx, hidden, weights):
    vm = pl.BlockSpec(memory_space=pltpu.VMEM)
    return pl.pallas_call(
        down_kernel,
        in_specs=[pl.BlockSpec(memory_space=pltpu.SMEM)] + [vm] * 5,
        out_specs=vm,
        out_shape=jax.ShapeDtypeStruct((CHUNK, COLS), BF16),
        name="down",
    )(idx, hidden, *weights)


def mix_kernel(idx_ref, r_ref, x_ref, stat_ref, gain_ref, bias_ref, scale_ref, mixed_ref, part_ref):
    branch = jnp.zeros((16, COLS), F32)
    for k in range(16):
        branch = branch + r_ref[k].astype(F32)
    mine = iota((16, ROWS), 1) == iota((16, ROWS), 0) + idx_ref[2]
    mean = jnp.sum(jnp.where(mine, stat_ref[0:1], 0.0), axis=1, keepdims=True)
    rstd = jnp.sum(jnp.where(mine, stat_ref[1:2], 0.0), axis=1, keepdims=True)
    normed = rounded((x_ref[0].astype(F32) - mean) * rstd * gain_ref[...] + bias_ref[...])
    mixed = 0.5 * normed + branch * scale_ref[...]
    mixed_ref[...] = mixed
    m = jnp.sum(mixed, axis=1, keepdims=True) * (1.0 / COLS)
    c = mixed - m
    m2 = jnp.sum(c * c, axis=1, keepdims=True)
    lane = iota((16, 128), 1)
    part = jnp.where(lane == 0, m, jnp.where(lane == 1, m2, 0.0))
    for k in range(4):
        part_ref[k] = part


def mix(idx, received, tokens, stats, gain, bias, scale):
    row = pl.BlockSpec((1, COLS), lambda i, s: (0, 0))
    return pl.pallas_call(
        mix_kernel,
        grid_spec=pltpu.PrefetchScalarGridSpec(
            num_scalar_prefetch=1,
            grid=(1,),
            in_specs=[
                pl.BlockSpec((16, 16, COLS), lambda i, s: (0, 0, 0)),
                pl.BlockSpec((1, 16, COLS), lambda i, s: (s[3], 0, 0)),
                pl.BlockSpec((8, ROWS), lambda i, s: (0, 0)),
                row,
                row,
                row,
            ],
            out_specs=[
                pl.BlockSpec((16, COLS), lambda i, s: (0, 0)),
                pl.BlockSpec((4, 16, 128), lambda i, s: (0, 0, 0)),
            ],
        ),
        out_shape=[jax.ShapeDtypeStruct((16, COLS), F32), jax.ShapeDtypeStruct((4, 16, 128), F32)],
        name="mix",
    )(idx, received, tokens.reshape(64, 16, COLS), stats, gain, bias, scale)


def finish_kernel(mixed_ref, part_ref, gain_ref, bias_ref, out_ref):
    parts = [part_ref[k] for k in range(4)]
    means = [p[:, 0:1] for p in parts]
    mean = (means[0] + means[1] + means[2] + means[3]) * 0.25
    m2 = sum(p[:, 1:2] for p in parts) + COLS * sum((v - mean) * (v - mean) for v in means)
    rstd = lax.rsqrt(m2 * (1.0 / D) + 1e-05)
    out_ref[...] = ((mixed_ref[...] - mean) * rstd * gain_ref[...] + bias_ref[...]).astype(BF16)


def finish(mixed, parts, gain, bias):
    vm = pl.BlockSpec(memory_space=pltpu.VMEM)
    return pl.pallas_call(
        finish_kernel,
        in_specs=[vm] * 4,
        out_specs=vm,
        out_shape=jax.ShapeDtypeStruct((16, COLS), BF16),
        name="finish",
    )(mixed, parts, gain, bias)


def swapped(n, k):
    return [(i, i ^ k) for i in range(n)]


def local(
    tokens,
    norm_gain,
    norm_bias,
    gate_weight,
    up_weight,
    gate_scale,
    up_scale,
    down_weight,
    down_scale,
    out_gain,
    out_bias,
):
    x_at = lax.axis_index("cb")
    member = lax.axis_index(("zl", "yl"))
    block = lax.axis_index(("Z", "Y"))
    idx = jnp.stack([x_at, member, member * CHUNK + block * 16, lax.axis_index(RA)]).astype(jnp.int32)
    gain = norm_gain.reshape(1, COLS)
    bias = norm_bias.reshape(1, COLS)

    w0 = down_weight.astype(BF16)
    w1 = lax.ppermute(w0, "yl", swapped(2, 1))
    w2 = lax.ppermute(w0, "zl", swapped(2, 1))
    w3 = lax.ppermute(w0, ("zl", "yl"), swapped(4, 3))

    shares = project(tokens, gate_weight.T, up_weight.T, gain, bias)
    received = lax.all_to_all(shares, "cb", 0, 0, tiled=True)
    sent, stats = hidden_of(idx, received, gate_scale.reshape(1, FFL), up_scale.reshape(1, FFL))
    hidden = lax.all_to_all(sent.reshape(16, SLOT, CHUNK), ("zl", "yl", "cb"), 0, 0, tiled=True)
    partial = down(idx, hidden.reshape(4, 4 * SLOT, CHUNK), (w0, w1, w2, w3))
    pieces = lax.all_to_all(partial.reshape(16, 16, COLS), ("Z", "Y"), 0, 0, tiled=True)
    mixed, part = mix(idx, pieces, tokens, stats, gain, bias, down_scale.reshape(1, COLS))
    parts = lax.all_to_all(part, "cb", 0, 0, tiled=True)
    return finish(mixed, parts, out_gain.reshape(1, COLS), out_bias.reshape(1, COLS))


def solution(mesh):
    split = Mesh(mesh.devices.reshape(4, 2, 4, 2, 4, 2), RA + ("cb", "dp"))
    return jax.shard_map(
        local,
        mesh=split,
        in_specs=(
            P("dp", "cb"),
            P("cb"),
            P("cb"),
            P("cb", RA),
            P("cb", RA),
            P(RA),
            P(RA),
            P(RA, "cb"),
            P("cb"),
            P("cb"),
            P("cb"),
        ),
        out_specs=P(("dp",) + RA, "cb"),
        check_vma=False,
    )
```

```python
import jax
import jax.numpy as jnp
from jax import lax
from jax.experimental import pallas as pl
from jax.experimental.pallas import tpu as pltpu
from jax.sharding import Mesh, PartitionSpec as P


D = 4096
F32 = jnp.float32
BF16 = jnp.bfloat16
RA = ("Z", "zl", "Y", "yl")
UNITS = 44
SLOT = 48
PART = 2 * SLOT
ROWS = 1024
COLS = 1024
FFL = 176
CHUNK = 256


def iota(shape, dim):
    return lax.broadcasted_iota(jnp.int32, shape, dim)


def near(a):
    return pltpu.with_memory_space_constraint(a, pltpu.VMEM)


def dot(a, b, ca, cb):
    return lax.dot_general(a, b, (((ca,), (cb,)), ((), ())), preferred_element_type=F32)


def rounded(v):
    return v.astype(BF16).astype(F32)


def one_hot(cond):
    return jnp.where(cond, 1.0, 0.0).astype(BF16)


def project_kernel(x_ref, gw_ref, uw_ref, gain_ref, bias_ref, out_ref, w_ref, vec_ref):
    step = pl.program_id(0)

    @pl.when(step == 0)
    def _():
        gw = gw_ref[...].astype(BF16)
        uw = uw_ref[...].astype(BF16)
        row = iota((PART, FFL), 0)
        col = iota((PART, FFL), 1)
        for k in range(4):
            unit = col - UNITS * k
            as_gate = one_hot((unit == row) & (row < UNITS))
            as_up = one_hot((unit == row - SLOT) & (row >= SLOT) & (row < SLOT + UNITS))
            w = dot(as_gate, gw, 1, 0) + dot(as_up, uw, 1, 0)
            w_ref[PART * k : PART * (k + 1), :] = w.astype(BF16)
        gain = gain_ref[...]
        bias = bias_ref[...]
        r = iota((8, COLS), 0)
        gh = rounded(gain)
        bh = rounded(bias)
        lead = jnp.where(r == 0, gh, jnp.where(r == 1, gain - gh, jnp.where(r == 2, bh, jnp.where(r == 3, bias - bh, 0.0))))
        sums = dot(lead.astype(BF16), w_ref[...], 1, 1)
        both = jnp.concatenate(
            [sums[0:1] + sums[1:2], sums[2:3] + sums[3:4], jnp.zeros((1, ROWS - 8 * PART), F32)], axis=1
        )
        hi = rounded(both)
        q = iota((8, ROWS), 0)
        vec_ref[...] = jnp.where(q == 0, hi, jnp.where(q == 1, both - hi, 0.0))

    x = x_ref[...].reshape(CHUNK, COLS).astype(F32)
    m = jnp.sum(x, axis=1, keepdims=True) * (1.0 / COLS)
    xc = x - m
    m2 = jnp.sum(xc * xc, axis=1, keepdims=True)
    xn = (xc * gain_ref[...]).astype(BF16)
    part = dot(w_ref[...], xn, 1, 1)
    lane = iota((CHUNK, 128), 1)
    stat = jnp.where(lane == 0, m, jnp.where(lane == 1, m2, 0.0)).T
    m_row = stat[0:1]
    m2_row = stat[1:2]
    m_hi = rounded(m_row)
    m_mid = rounded(m_row - m_hi)
    m_lo = m_row - m_hi - m_mid
    m2_hi = rounded(m2_row)
    m2_lo = m2_row - m2_hi
    vec = vec_ref[:, pl.ds(pl.multiple_of(step * CHUNK, CHUNK), CHUNK)]
    r = iota((8, CHUNK), 0)
    t1 = jnp.where(r == 4, m_hi, jnp.where(r == 5, m_mid, jnp.where(r == 6, m_lo, jnp.where(r == 7, vec[0:1], 0.0))))
    t2 = jnp.where(r == 4, m2_hi, jnp.where(r == 5, m2_lo, jnp.where(r == 6, vec[1:2], 0.0)))
    z = jnp.zeros((SLOT - 8, CHUNK), F32)
    extra = jnp.concatenate([z, t1, z, t2], axis=0)
    for k in range(4):
        out_ref[k] = (part[PART * k : PART * (k + 1)] + extra).astype(BF16)


def project(tokens, gate_t, up_t, gain, bias):
    x = tokens.reshape(4, 2, 4, 2, 16, COLS)
    return pl.pallas_call(
        project_kernel,
        grid=(4,),
        in_specs=[
            pl.BlockSpec((4, 1, 4, 1, 16, COLS), lambda j: (0, j // 2, 0, j % 2, 0, 0)),
            pl.BlockSpec((FFL, COLS), lambda j: (0, 0)),
            pl.BlockSpec((FFL, COLS), lambda j: (0, 0)),
            pl.BlockSpec((1, COLS), lambda j: (0, 0)),
            pl.BlockSpec((1, COLS), lambda j: (0, 0)),
        ],
        out_specs=pl.BlockSpec((4, PART, CHUNK), lambda j: (0, 0, j)),
        out_shape=jax.ShapeDtypeStruct((4, PART, ROWS), BF16),
        scratch_shapes=[pltpu.VMEM((4 * PART, COLS), BF16), pltpu.VMEM((8, ROWS), F32)],
        compiler_params=pltpu.CompilerParams(dimension_semantics=("arbitrary",)),
        name="project",
    )(x, gate_t, up_t, gain, bias)


def hidden_kernel(idx_ref, r_ref, gs_ref, us_ref, out_ref, stat_ref):
    me = idx_ref[0]
    means = []
    m2s = []
    for c in range(4):
        a = r_ref[c, 32:48, :].astype(F32)
        b = r_ref[c, 80:96, :].astype(F32)
        means.append(a[12:13] + a[13:14] + a[14:15])
        m2s.append(b[12:13] + b[13:14])
    mean = (means[0] + means[1] + means[2] + means[3]) * 0.25
    deltas = [v - mean for v in means]
    m2 = sum(m2s) + COLS * sum(d * d for d in deltas)
    rstd = lax.rsqrt(m2 * (1.0 / D) + 1e-05)
    q = iota((8, ROWS), 0)
    stat_ref[...] = jnp.where(q == 0, mean, jnp.where(q == 1, rstd, 0.0))

    wide = 8 * PART
    pick_row = iota((2 * PART, wide), 0)
    pick_lane = iota((2 * PART, wide), 1)
    base = jnp.where(pick_row < PART, me * PART, (4 + me) * PART - PART)
    pick = one_hot(pick_lane == pick_row + base)
    tiles = [r_ref[c, 32:48, 0:wide] for c in range(4)] + [r_ref[c, 80:96, 0:wide] for c in range(4)]
    vecs = dot(pick, jnp.concatenate(tiles, axis=0), 1, 1)
    col_sums = [vecs[0:PART, 16 * c + 15 : 16 * c + 16] + vecs[0:PART, 78 + 16 * c : 79 + 16 * c] for c in range(4)]
    biases = sum(vecs[PART:, 16 * c + 15 : 16 * c + 16] + vecs[PART:, 78 + 16 * c : 79 + 16 * c] for c in range(4))

    gs = gs_ref[...]
    us = us_ref[...]
    g1 = rounded(gs)
    g2 = rounded(gs - g1)
    u1 = rounded(us)
    u2 = rounded(us - u1)
    sr = iota((16, FFL), 0)
    pieces = jnp.where(sr == 0, g1, jnp.where(sr == 1, g2, jnp.where(sr == 2, gs - g1 - g2, 0.0)))
    pieces = pieces + jnp.where(sr == 3, u1, jnp.where(sr == 4, u2, jnp.where(sr == 5, us - u1 - u2, 0.0)))
    row = iota((PART, FFL), 0)
    unit = jnp.where(row < SLOT, row, row - SLOT)
    own = one_hot((iota((PART, FFL), 1) == unit + me * UNITS) & (unit < UNITS))
    sc = dot(own, pieces.astype(BF16), 1, 1)
    scale = jnp.where(iota((PART, 1), 0) < SLOT, sc[:, 0:1] + sc[:, 1:2] + sc[:, 2:3], sc[:, 3:4] + sc[:, 4:5] + sc[:, 5:6])

    keep = iota((SLOT, CHUNK), 0) < UNITS
    for j in range(4):
        at = slice(CHUNK * j, CHUNK * (j + 1))
        acc = jnp.zeros((PART, CHUNK), F32)
        for c in range(4):
            acc = acc + (r_ref[c, :, at].astype(F32) + col_sums[c] * deltas[c][:, at])
        y = (acc * rstd[:, at] + biases) * scale
        gate = y[0:SLOT]
        up = y[SLOT:PART]
        h = jnp.where(keep, gate / (1.0 + jnp.exp(-gate)) * up, 0.0).astype(BF16)
        for k in range(4):
            out_ref[j, k] = h


def hidden_of(idx, received, gate_scale, up_scale):
    vm = pl.BlockSpec(memory_space=pltpu.VMEM)
    return pl.pallas_call(
        hidden_kernel,
        in_specs=[pl.BlockSpec(memory_space=pltpu.SMEM), vm, vm, vm],
        out_specs=[vm, vm],
        out_shape=[pltpu.VMEM((4, 4, SLOT, CHUNK), BF16), pltpu.VMEM((8, ROWS), F32)],
        name="hidden",
    )(idx, *[near(a) for a in (received, gate_scale, up_scale)])


def down_kernel(idx_ref, h_ref, w0_ref, w1_ref, w2_ref, w3_ref, out_ref):
    me = idx_ref[1]
    row = iota((FFL, 4 * SLOT), 0)
    lane = iota((FFL, 4 * SLOT), 1)
    hit = lane < 0
    for k in range(4):
        hit = hit | ((lane == row + (SLOT - UNITS) * k) & (row >= UNITS * k) & (row < UNITS * (k + 1)))
    squeeze = one_hot(hit)
    acc = jnp.zeros((CHUNK, COLS), F32)
    for r, w_ref in enumerate((w0_ref, w1_ref, w2_ref, w3_ref)):
        h = dot(h_ref[me ^ r], squeeze, 0, 1).astype(BF16)
        acc = acc + dot(h, w_ref[...], 1, 0)
    out_ref[...] = acc.astype(BF16)


def down(idx, hidden, weights):
    vm = pl.BlockSpec(memory_space=pltpu.VMEM)
    return pl.pallas_call(
        down_kernel,
        in_specs=[pl.BlockSpec(memory_space=pltpu.SMEM)] + [vm] * 5,
        out_specs=vm,
        out_shape=pltpu.VMEM((CHUNK, COLS), BF16),
        name="down",
    )(idx, near(hidden), *[near(w) for w in weights])


def mix_kernel(idx_ref, r_ref, x_ref, stat_ref, gain_ref, bias_ref, scale_ref, mixed_ref, part_ref):
    branch = jnp.zeros((16, COLS), F32)
    for k in range(16):
        branch = branch + r_ref[k].astype(F32)
    mine = iota((16, ROWS), 1) == iota((16, ROWS), 0) + idx_ref[2]
    mean = jnp.sum(jnp.where(mine, stat_ref[0:1], 0.0), axis=1, keepdims=True)
    rstd = jnp.sum(jnp.where(mine, stat_ref[1:2], 0.0), axis=1, keepdims=True)
    normed = rounded((x_ref[...].astype(F32) - mean) * rstd * gain_ref[...] + bias_ref[...])
    mixed = 0.5 * normed + branch * scale_ref[...]
    mixed_ref[...] = mixed
    m = jnp.sum(mixed, axis=1, keepdims=True) * (1.0 / COLS)
    c = mixed - m
    m2 = jnp.sum(c * c, axis=1, keepdims=True)
    lane = iota((16, 128), 1)
    part = jnp.where(lane == 0, m, jnp.where(lane == 1, m2, 0.0))
    for k in range(4):
        part_ref[k] = part


def mix(idx, received, own, stats, gain, bias, scale):
    vm = pl.BlockSpec(memory_space=pltpu.VMEM)
    return pl.pallas_call(
        mix_kernel,
        in_specs=[pl.BlockSpec(memory_space=pltpu.SMEM)] + [vm] * 6,
        out_specs=[vm, vm],
        out_shape=[pltpu.VMEM((16, COLS), F32), pltpu.VMEM((4, 16, 128), F32)],
        name="mix",
    )(idx, *[near(a) for a in (received, own, stats, gain, bias, scale)])


def finish_kernel(mixed_ref, part_ref, gain_ref, bias_ref, out_ref):
    parts = [part_ref[k] for k in range(4)]
    means = [p[:, 0:1] for p in parts]
    mean = (means[0] + means[1] + means[2] + means[3]) * 0.25
    m2 = sum(p[:, 1:2] for p in parts) + COLS * sum((v - mean) * (v - mean) for v in means)
    rstd = lax.rsqrt(m2 * (1.0 / D) + 1e-05)
    out_ref[...] = ((mixed_ref[...] - mean) * rstd * gain_ref[...] + bias_ref[...]).astype(BF16)


def finish(mixed, parts, gain, bias):
    vm = pl.BlockSpec(memory_space=pltpu.VMEM)
    return pl.pallas_call(
        finish_kernel,
        in_specs=[vm] * 4,
        out_specs=vm,
        out_shape=jax.ShapeDtypeStruct((16, COLS), BF16),
        name="finish",
    )(*[near(a) for a in (mixed, parts, gain, bias)])


def swapped(n, k):
    return [(i, i ^ k) for i in range(n)]


def local(
    tokens,
    norm_gain,
    norm_bias,
    gate_weight,
    up_weight,
    gate_scale,
    up_scale,
    down_weight,
    down_scale,
    out_gain,
    out_bias,
):
    x_at = lax.axis_index("cb")
    member = lax.axis_index(("zl", "yl"))
    block = lax.axis_index(("Z", "Y"))
    idx = jnp.stack([x_at, member, member * CHUNK + block * 16]).astype(jnp.int32)
    gain = norm_gain.reshape(1, COLS)
    bias = norm_bias.reshape(1, COLS)

    w0 = down_weight.astype(BF16)
    w1 = lax.ppermute(w0, "yl", swapped(2, 1))
    w2 = lax.ppermute(w0, "zl", swapped(2, 1))
    w3 = lax.ppermute(w0, ("zl", "yl"), swapped(4, 3))

    shares = project(tokens, gate_weight.T, up_weight.T, gain, bias)
    received = lax.all_to_all(shares, "cb", 0, 0, tiled=True)
    sent, stats = hidden_of(idx, received, gate_scale.reshape(1, FFL), up_scale.reshape(1, FFL))
    own = lax.dynamic_slice_in_dim(tokens, lax.axis_index(RA) * 16, 16, 0)
    sent, own = lax.optimization_barrier((sent, own))
    hidden = lax.all_to_all(sent.reshape(16, SLOT, CHUNK), ("zl", "yl", "cb"), 0, 0, tiled=True)
    partial = down(idx, hidden.reshape(4, 4 * SLOT, CHUNK), (w0, w1, w2, w3))
    pieces = lax.all_to_all(partial.reshape(16, 16, COLS), ("Z", "Y"), 0, 0, tiled=True)
    mixed, part = mix(idx, pieces, own, stats, gain, bias, down_scale.reshape(1, COLS))
    parts = lax.all_to_all(part, "cb", 0, 0, tiled=True)
    return finish(mixed, parts, out_gain.reshape(1, COLS), out_bias.reshape(1, COLS))


def solution(mesh):
    split = Mesh(mesh.devices.reshape(4, 2, 4, 2, 4, 2), RA + ("cb", "dp"))
    return jax.shard_map(
        local,
        mesh=split,
        in_specs=(
            P("dp", "cb"),
            P("cb"),
            P("cb"),
            P("cb", RA),
            P("cb", RA),
            P(RA),
            P(RA),
            P(RA, "cb"),
            P("cb"),
            P("cb"),
            P("cb"),
        ),
        out_specs=P(("dp",) + RA, "cb"),
        check_vma=False,
    )
```

```python
import jax
import jax.numpy as jnp
from jax import lax
from jax.experimental import pallas as pl
from jax.experimental.pallas import tpu as pltpu
from jax.sharding import Mesh, PartitionSpec as P


D = 4096
F32 = jnp.float32
BF16 = jnp.bfloat16
RA = ("Z", "zl", "Y", "yl")
UNITS = 44
SLOT = 48
PART = 2 * SLOT
ROWS = 1024
COLS = 1024
FFL = 176
CHUNK = 256


def iota(shape, dim):
    return lax.broadcasted_iota(jnp.int32, shape, dim)


def near(a):
    return pltpu.with_memory_space_constraint(a, pltpu.VMEM)


def dot(a, b, ca, cb):
    return lax.dot_general(a, b, (((ca,), (cb,)), ((), ())), preferred_element_type=F32)


def rounded(v):
    return v.astype(BF16).astype(F32)


def one_hot(cond):
    return jnp.where(cond, 1.0, 0.0).astype(BF16)


def project_kernel(x_ref, gw_ref, uw_ref, gain_ref, bias_ref, out_ref, w_ref, vec_ref):
    step = pl.program_id(0)

    @pl.when(step == 0)
    def _():
        gw = gw_ref[...].astype(BF16)
        uw = uw_ref[...].astype(BF16)
        row = iota((PART, FFL), 0)
        col = iota((PART, FFL), 1)
        for k in range(4):
            unit = col - UNITS * k
            as_gate = one_hot((unit == row) & (row < UNITS))
            as_up = one_hot((unit == row - SLOT) & (row >= SLOT) & (row < SLOT + UNITS))
            w = dot(as_gate, gw, 1, 0) + dot(as_up, uw, 1, 0)
            w_ref[PART * k : PART * (k + 1), :] = w.astype(BF16)
        gain = gain_ref[...]
        bias = bias_ref[...]
        r = iota((8, COLS), 0)
        gh = rounded(gain)
        bh = rounded(bias)
        lead = jnp.where(r == 0, gh, jnp.where(r == 1, gain - gh, jnp.where(r == 2, bh, jnp.where(r == 3, bias - bh, 0.0))))
        sums = dot(lead.astype(BF16), w_ref[...], 1, 1)
        both = jnp.concatenate(
            [sums[0:1] + sums[1:2], sums[2:3] + sums[3:4], jnp.zeros((1, ROWS - 8 * PART), F32)], axis=1
        )
        hi = rounded(both)
        q = iota((8, ROWS), 0)
        vec_ref[...] = jnp.where(q == 0, hi, jnp.where(q == 1, both - hi, 0.0))

    x = x_ref[...].reshape(CHUNK, COLS).astype(F32)
    m = jnp.sum(x, axis=1, keepdims=True) * (1.0 / COLS)
    xc = x - m
    m2 = jnp.sum(xc * xc, axis=1, keepdims=True)
    xn = (xc * gain_ref[...]).astype(BF16)
    part = dot(w_ref[...], xn, 1, 1)
    lane = iota((CHUNK, 128), 1)
    stat = jnp.where(lane == 0, m, jnp.where(lane == 1, m2, 0.0)).T
    m_row = stat[0:1]
    m2_row = stat[1:2]
    m_hi = rounded(m_row)
    m_mid = rounded(m_row - m_hi)
    m_lo = m_row - m_hi - m_mid
    m2_hi = rounded(m2_row)
    m2_lo = m2_row - m2_hi
    vec = vec_ref[:, pl.ds(pl.multiple_of(step * CHUNK, CHUNK), CHUNK)]
    r = iota((8, CHUNK), 0)
    t1 = jnp.where(r == 4, m_hi, jnp.where(r == 5, m_mid, jnp.where(r == 6, m_lo, jnp.where(r == 7, vec[0:1], 0.0))))
    t2 = jnp.where(r == 4, m2_hi, jnp.where(r == 5, m2_lo, jnp.where(r == 6, vec[1:2], 0.0)))
    z = jnp.zeros((SLOT - 8, CHUNK), F32)
    extra = jnp.concatenate([z, t1, z, t2], axis=0)
    for k in range(4):
        out_ref[k] = (part[PART * k : PART * (k + 1)] + extra).astype(BF16)


def project(tokens, gate_t, up_t, gain, bias):
    x = tokens.reshape(4, 2, 4, 2, 16, COLS)
    return pl.pallas_call(
        project_kernel,
        grid=(4,),
        in_specs=[
            pl.BlockSpec((4, 1, 4, 1, 16, COLS), lambda j: (0, j // 2, 0, j % 2, 0, 0)),
            pl.BlockSpec((FFL, COLS), lambda j: (0, 0)),
            pl.BlockSpec((FFL, COLS), lambda j: (0, 0)),
            pl.BlockSpec((1, COLS), lambda j: (0, 0)),
            pl.BlockSpec((1, COLS), lambda j: (0, 0)),
        ],
        out_specs=pl.BlockSpec((4, PART, CHUNK), lambda j: (0, 0, j)),
        out_shape=jax.ShapeDtypeStruct((4, PART, ROWS), BF16),
        scratch_shapes=[pltpu.VMEM((4 * PART, COLS), BF16), pltpu.VMEM((8, ROWS), F32)],
        compiler_params=pltpu.CompilerParams(dimension_semantics=("arbitrary",)),
        name="project",
    )(x, gate_t, up_t, gain, bias)


def hidden_kernel(r_ref, gs_ref, us_ref, out_ref, stat_ref):
    me = lax.axis_index("cb")
    means = []
    m2s = []
    for c in range(4):
        a = r_ref[c, 32:48, :].astype(F32)
        b = r_ref[c, 80:96, :].astype(F32)
        means.append(a[12:13] + a[13:14] + a[14:15])
        m2s.append(b[12:13] + b[13:14])
    mean = (means[0] + means[1] + means[2] + means[3]) * 0.25
    deltas = [v - mean for v in means]
    m2 = sum(m2s) + COLS * sum(d * d for d in deltas)
    rstd = lax.rsqrt(m2 * (1.0 / D) + 1e-05)
    q = iota((8, ROWS), 0)
    stat_ref[...] = jnp.where(q == 0, mean, jnp.where(q == 1, rstd, 0.0))

    wide = 8 * PART
    pick_row = iota((2 * PART, wide), 0)
    pick_lane = iota((2 * PART, wide), 1)
    base = jnp.where(pick_row < PART, me * PART, (4 + me) * PART - PART)
    pick = one_hot(pick_lane == pick_row + base)
    tiles = [r_ref[c, 32:48, 0:wide] for c in range(4)] + [r_ref[c, 80:96, 0:wide] for c in range(4)]
    vecs = dot(pick, jnp.concatenate(tiles, axis=0), 1, 1)
    col_sums = [vecs[0:PART, 16 * c + 15 : 16 * c + 16] + vecs[0:PART, 78 + 16 * c : 79 + 16 * c] for c in range(4)]
    biases = sum(vecs[PART:, 16 * c + 15 : 16 * c + 16] + vecs[PART:, 78 + 16 * c : 79 + 16 * c] for c in range(4))

    gs = gs_ref[...]
    us = us_ref[...]
    g1 = rounded(gs)
    g2 = rounded(gs - g1)
    u1 = rounded(us)
    u2 = rounded(us - u1)
    sr = iota((16, FFL), 0)
    pieces = jnp.where(sr == 0, g1, jnp.where(sr == 1, g2, jnp.where(sr == 2, gs - g1 - g2, 0.0)))
    pieces = pieces + jnp.where(sr == 3, u1, jnp.where(sr == 4, u2, jnp.where(sr == 5, us - u1 - u2, 0.0)))
    row = iota((PART, FFL), 0)
    unit = jnp.where(row < SLOT, row, row - SLOT)
    own = one_hot((iota((PART, FFL), 1) == unit + me * UNITS) & (unit < UNITS))
    sc = dot(own, pieces.astype(BF16), 1, 1)
    scale = jnp.where(iota((PART, 1), 0) < SLOT, sc[:, 0:1] + sc[:, 1:2] + sc[:, 2:3], sc[:, 3:4] + sc[:, 4:5] + sc[:, 5:6])

    keep = iota((SLOT, CHUNK), 0) < UNITS
    for j in range(4):
        at = slice(CHUNK * j, CHUNK * (j + 1))
        acc = jnp.zeros((PART, CHUNK), F32)
        for c in range(4):
            acc = acc + (r_ref[c, :, at].astype(F32) + col_sums[c] * deltas[c][:, at])
        y = (acc * rstd[:, at] + biases) * scale
        gate = y[0:SLOT]
        up = y[SLOT:PART]
        h = jnp.where(keep, gate / (1.0 + jnp.exp(-gate)) * up, 0.0).astype(BF16)
        for k in range(4):
            out_ref[j, k] = h


def hidden_of(received, gate_scale, up_scale):
    vm = pl.BlockSpec(memory_space=pltpu.VMEM)
    return pl.pallas_call(
        hidden_kernel,
        in_specs=[vm, vm, vm],
        out_specs=[vm, vm],
        out_shape=[pltpu.VMEM((4, 4, SLOT, CHUNK), BF16), pltpu.VMEM((8, ROWS), F32)],
        name="hidden",
    )(*[near(a) for a in (received, gate_scale, up_scale)])


def down_kernel(h_ref, w0_ref, w1_ref, w2_ref, w3_ref, out_ref):
    me = lax.axis_index("zl") * 2 + lax.axis_index("yl")
    row = iota((FFL, 4 * SLOT), 0)
    lane = iota((FFL, 4 * SLOT), 1)
    hit = lane < 0
    for k in range(4):
        hit = hit | ((lane == row + (SLOT - UNITS) * k) & (row >= UNITS * k) & (row < UNITS * (k + 1)))
    squeeze = one_hot(hit)
    acc = jnp.zeros((CHUNK, COLS), F32)
    for r, w_ref in enumerate((w0_ref, w1_ref, w2_ref, w3_ref)):
        h = dot(h_ref[me ^ r], squeeze, 0, 1).astype(BF16)
        acc = acc + dot(h, w_ref[...], 1, 0)
    out_ref[...] = acc.astype(BF16)


def down(hidden, weights):
    vm = pl.BlockSpec(memory_space=pltpu.VMEM)
    return pl.pallas_call(
        down_kernel,
        in_specs=[vm] * 5,
        out_specs=vm,
        out_shape=pltpu.VMEM((CHUNK, COLS), BF16),
        name="down",
    )(near(hidden), *[near(w) for w in weights])


def mix_kernel(r_ref, x_ref, stat_ref, gain_ref, bias_ref, scale_ref, mixed_ref, part_ref):
    member = lax.axis_index("zl") * 2 + lax.axis_index("yl")
    at = member * CHUNK + (lax.axis_index("Z") * 4 + lax.axis_index("Y")) * 16
    branch = jnp.zeros((16, COLS), F32)
    for k in range(16):
        branch = branch + r_ref[k].astype(F32)
    mine = iota((16, ROWS), 1) == iota((16, ROWS), 0) + at
    mean = jnp.sum(jnp.where(mine, stat_ref[0:1], 0.0), axis=1, keepdims=True)
    rstd = jnp.sum(jnp.where(mine, stat_ref[1:2], 0.0), axis=1, keepdims=True)
    normed = rounded((x_ref[...].astype(F32) - mean) * rstd * gain_ref[...] + bias_ref[...])
    mixed = 0.5 * normed + branch * scale_ref[...]
    mixed_ref[...] = mixed
    m = jnp.sum(mixed, axis=1, keepdims=True) * (1.0 / COLS)
    c = mixed - m
    m2 = jnp.sum(c * c, axis=1, keepdims=True)
    lane = iota((16, 128), 1)
    part = jnp.where(lane == 0, m, jnp.where(lane == 1, m2, 0.0))
    for k in range(4):
        part_ref[k] = part


def mix(received, own, stats, gain, bias, scale):
    vm = pl.BlockSpec(memory_space=pltpu.VMEM)
    return pl.pallas_call(
        mix_kernel,
        in_specs=[vm] * 6,
        out_specs=[vm, vm],
        out_shape=[pltpu.VMEM((16, COLS), F32), pltpu.VMEM((4, 16, 128), F32)],
        name="mix",
    )(*[near(a) for a in (received, own, stats, gain, bias, scale)])


def finish_kernel(mixed_ref, part_ref, gain_ref, bias_ref, out_ref):
    parts = [part_ref[k] for k in range(4)]
    means = [p[:, 0:1] for p in parts]
    mean = (means[0] + means[1] + means[2] + means[3]) * 0.25
    m2 = sum(p[:, 1:2] for p in parts) + COLS * sum((v - mean) * (v - mean) for v in means)
    rstd = lax.rsqrt(m2 * (1.0 / D) + 1e-05)
    out_ref[...] = ((mixed_ref[...] - mean) * rstd * gain_ref[...] + bias_ref[...]).astype(BF16)


def finish(mixed, parts, gain, bias):
    vm = pl.BlockSpec(memory_space=pltpu.VMEM)
    return pl.pallas_call(
        finish_kernel,
        in_specs=[vm] * 4,
        out_specs=vm,
        out_shape=jax.ShapeDtypeStruct((16, COLS), BF16),
        name="finish",
    )(*[near(a) for a in (mixed, parts, gain, bias)])


def swapped(n, k):
    return [(i, i ^ k) for i in range(n)]


def local(
    tokens,
    norm_gain,
    norm_bias,
    gate_weight,
    up_weight,
    gate_scale,
    up_scale,
    down_weight,
    down_scale,
    out_gain,
    out_bias,
):
    gain = norm_gain.reshape(1, COLS)
    bias = norm_bias.reshape(1, COLS)

    w0 = down_weight.astype(BF16)
    w1 = lax.ppermute(w0, "yl", swapped(2, 1))
    w2 = lax.ppermute(w0, "zl", swapped(2, 1))
    w3 = lax.ppermute(w0, ("zl", "yl"), swapped(4, 3))

    shares = project(tokens, gate_weight.T, up_weight.T, gain, bias)
    received = lax.all_to_all(shares, "cb", 0, 0, tiled=True)
    sent, stats = hidden_of(received, gate_scale.reshape(1, FFL), up_scale.reshape(1, FFL))
    hidden = lax.all_to_all(sent.reshape(16, SLOT, CHUNK), ("zl", "yl", "cb"), 0, 0, tiled=True)
    own = lax.dynamic_slice_in_dim(tokens, lax.axis_index(RA) * 16, 16, 0)
    hidden, own = lax.optimization_barrier((hidden, own))
    partial = down(hidden.reshape(4, 4 * SLOT, CHUNK), (w0, w1, w2, w3))
    pieces = lax.all_to_all(partial.reshape(16, 16, COLS), ("Z", "Y"), 0, 0, tiled=True)
    mixed, part = mix(pieces, own, stats, gain, bias, down_scale.reshape(1, COLS))
    parts = lax.all_to_all(part, "cb", 0, 0, tiled=True)
    return finish(mixed, parts, out_gain.reshape(1, COLS), out_bias.reshape(1, COLS))


def solution(mesh):
    split = Mesh(mesh.devices.reshape(4, 2, 4, 2, 4, 2), RA + ("cb", "dp"))
    return jax.shard_map(
        local,
        mesh=split,
        in_specs=(
            P("dp", "cb"),
            P("cb"),
            P("cb"),
            P("cb", RA),
            P("cb", RA),
            P(RA),
            P(RA),
            P(RA, "cb"),
            P("cb"),
            P("cb"),
            P("cb"),
        ),
        out_specs=P(("dp",) + RA, "cb"),
        check_vma=False,
    )
```

```python
import jax
import jax.numpy as jnp
from jax import lax
from jax.experimental import pallas as pl
from jax.experimental.pallas import tpu as pltpu
from jax.sharding import Mesh, PartitionSpec as P


D = 4096
F32 = jnp.float32
BF16 = jnp.bfloat16
RA = ("Z", "zl", "Y", "yl")
UNITS = 44
SLOT = 48
PART = 2 * SLOT
ROWS = 1024
COLS = 1024
FFL = 176
CHUNK = 256


def iota(shape, dim):
    return lax.broadcasted_iota(jnp.int32, shape, dim)


def near(a):
    return pltpu.with_memory_space_constraint(a, pltpu.VMEM)


def dot(a, b, ca, cb):
    return lax.dot_general(a, b, (((ca,), (cb,)), ((), ())), preferred_element_type=F32)


def rounded(v):
    return v.astype(BF16).astype(F32)


def one_hot(cond):
    return jnp.where(cond, 1.0, 0.0).astype(BF16)


def project_kernel(x_ref, gw_ref, uw_ref, gain_ref, bias_ref, out_ref, x_buf, gw_buf, uw_buf, gb_buf, out_buf, w_ref, vec_ref, sems):
    loads = [
        pltpu.make_async_copy(gw_ref, gw_buf, sems.at[0]),
        pltpu.make_async_copy(uw_ref, uw_buf, sems.at[1]),
        pltpu.make_async_copy(gain_ref, gb_buf.at[0], sems.at[2]),
        pltpu.make_async_copy(bias_ref, gb_buf.at[1], sems.at[3]),
    ]
    tokens = [pltpu.make_async_copy(x_ref.at[:, j // 2, :, j % 2], x_buf.at[j], sems.at[4 + j]) for j in range(4)]
    for copy in loads + tokens[:1]:
        copy.start()
    for copy in loads:
        copy.wait()
    for copy in tokens[1:]:
        copy.start()

    gain = gb_buf[0]
    row = iota((SLOT, COLS), 0)
    for k in range(4):
        first = UNITS * k - 4 * (k % 2)
        for half, ref in enumerate((gw_buf, uw_buf)):
            w = ref[first : min(first + SLOT + 8 * (k % 2), FFL)] * gain
            if k % 2:
                w = pltpu.roll(w, w.shape[0] - 4, 0)
            fill = jnp.where(row == UNITS, 1.0, 0.0) if half == 0 else 0.0
            at = PART * k + SLOT * half
            w_ref[at : at + SLOT, :] = jnp.where(row < UNITS, w[0:SLOT], fill).astype(BF16)
    r = iota((128, COLS), 0)
    ratio = gb_buf[1] / gain
    rh = rounded(ratio)
    lead = jnp.where(r == 0, 1.0, jnp.where(r == 1, rh, jnp.where(r == 2, ratio - rh, 0.0))).astype(BF16)
    cols = dot(w_ref[...], lead, 1, 1)
    col = cols[:, 0:1]
    sums = cols.T
    both = jnp.concatenate([sums[0:1], sums[1:2] + sums[2:3], jnp.zeros((1, ROWS - 8 * PART), F32)], axis=1)
    hi = rounded(both)
    q = iota((8, ROWS), 0)
    vec_ref[...] = jnp.where(q == 0, hi, jnp.where(q == 1, both - hi, 0.0))

    stores = []
    for j in range(4):
        at = slice(CHUNK * j, CHUNK * (j + 1))
        tokens[j].wait()
        part = dot(w_ref[...], x_buf[j].reshape(CHUNK, COLS), 1, 1)
        x = x_buf[j].reshape(CHUNK, COLS).astype(F32)
        pivot = x[:, 0:1]
        c = x - pivot
        sq = jnp.sum(c * c, axis=1, keepdims=True)
        lane = iota((CHUNK, 128), 1)
        stat = jnp.where(lane == 0, sq, jnp.where(lane == 1, pivot, 0.0)).T
        m_row = part[UNITS : UNITS + 1] * (1.0 / COLS)
        off = m_row - stat[1:2]
        m2_row = stat[0:1] - COLS * off * off
        m_hi = rounded(m_row)
        m_mid = rounded(m_row - m_hi)
        m_lo = m_row - m_hi - m_mid
        m2_hi = rounded(m2_row)
        m2_lo = m2_row - m2_hi
        r = iota((8, CHUNK), 0)
        t1 = jnp.where(r == 4, m_hi, jnp.where(r == 5, m_mid, jnp.where(r == 6, m_lo, jnp.where(r == 7, vec_ref[0:1, at], 0.0))))
        t2 = jnp.where(r == 4, m2_hi, jnp.where(r == 5, m2_lo, jnp.where(r == 6, vec_ref[1:2, at], 0.0)))
        z = jnp.zeros((SLOT - 8, CHUNK), F32)
        extra = jnp.concatenate([z, t1, z, t2], axis=0)
        for k in range(4):
            rows = slice(PART * k, PART * (k + 1))
            out_buf[k, :, at] = (part[rows] - col[rows] * m_row + extra).astype(BF16)
        stores.append(pltpu.make_async_copy(out_buf.at[:, :, at], out_ref.at[:, :, at], sems.at[8 + j]))
        stores[-1].start()
    for copy in stores:
        copy.wait()


def project(tokens, gate_t, up_t, gain, bias):
    hbm = pl.BlockSpec(memory_space=pl.ANY)
    return pl.pallas_call(
        project_kernel,
        in_specs=[hbm] * 5,
        out_specs=hbm,
        out_shape=pltpu.HBM((4, PART, ROWS), BF16),
        scratch_shapes=[
            pltpu.VMEM((4, 4, 4, 16, COLS), BF16),
            pltpu.VMEM((FFL, COLS), F32),
            pltpu.VMEM((FFL, COLS), F32),
            pltpu.VMEM((2, 1, COLS), F32),
            pltpu.VMEM((4, PART, ROWS), BF16),
            pltpu.VMEM((4 * PART, COLS), BF16),
            pltpu.VMEM((8, ROWS), F32),
            pltpu.SemaphoreType.DMA((12,)),
        ],
        name="project",
    )(*[pltpu.with_memory_space_constraint(a, pltpu.HBM) for a in (tokens.reshape(4, 2, 4, 2, 16, COLS), gate_t, up_t, gain, bias)])


def hidden_kernel(r_ref, gs_ref, us_ref, out_ref, stat_ref):
    me = lax.axis_index("cb")
    means = []
    m2s = []
    for c in range(4):
        a = r_ref[c, 32:48, :].astype(F32)
        b = r_ref[c, 80:96, :].astype(F32)
        means.append(a[12:13] + a[13:14] + a[14:15])
        m2s.append(b[12:13] + b[13:14])
    mean = (means[0] + means[1] + means[2] + means[3]) * 0.25
    deltas = [v - mean for v in means]
    m2 = sum(m2s) + COLS * sum(d * d for d in deltas)
    rstd = lax.rsqrt(m2 * (1.0 / D) + 1e-05)
    q = iota((8, ROWS), 0)
    stat_ref[...] = jnp.where(q == 0, mean, jnp.where(q == 1, rstd, 0.0))

    wide = 8 * PART
    pick_row = iota((2 * PART, wide), 0)
    pick_lane = iota((2 * PART, wide), 1)
    base = jnp.where(pick_row < PART, me * PART, (4 + me) * PART - PART)
    pick = one_hot(pick_lane == pick_row + base)
    tiles = [r_ref[c, 32:48, 0:wide] for c in range(4)] + [r_ref[c, 80:96, 0:wide] for c in range(4)]
    vecs = dot(pick, jnp.concatenate(tiles, axis=0), 1, 1)
    col_sums = [vecs[0:PART, 16 * c + 15 : 16 * c + 16] + vecs[0:PART, 78 + 16 * c : 79 + 16 * c] for c in range(4)]
    biases = sum(vecs[PART:, 16 * c + 15 : 16 * c + 16] + vecs[PART:, 78 + 16 * c : 79 + 16 * c] for c in range(4))

    gs = gs_ref[...]
    us = us_ref[...]
    g1 = rounded(gs)
    g2 = rounded(gs - g1)
    u1 = rounded(us)
    u2 = rounded(us - u1)
    sr = iota((16, FFL), 0)
    pieces = jnp.where(sr == 0, g1, jnp.where(sr == 1, g2, jnp.where(sr == 2, gs - g1 - g2, 0.0)))
    pieces = pieces + jnp.where(sr == 3, u1, jnp.where(sr == 4, u2, jnp.where(sr == 5, us - u1 - u2, 0.0)))
    row = iota((PART, FFL), 0)
    unit = jnp.where(row < SLOT, row, row - SLOT)
    own = one_hot((iota((PART, FFL), 1) == unit + me * UNITS) & (unit < UNITS))
    sc = dot(own, pieces.astype(BF16), 1, 1)
    scale = jnp.where(iota((PART, 1), 0) < SLOT, sc[:, 0:1] + sc[:, 1:2] + sc[:, 2:3], sc[:, 3:4] + sc[:, 4:5] + sc[:, 5:6])

    keep = iota((SLOT, CHUNK), 0) < UNITS
    for j in range(4):
        at = slice(CHUNK * j, CHUNK * (j + 1))
        acc = jnp.zeros((PART, CHUNK), F32)
        for c in range(4):
            acc = acc + (r_ref[c, :, at].astype(F32) + col_sums[c] * deltas[c][:, at])
        y = (acc * rstd[:, at] + biases) * scale
        gate = y[0:SLOT]
        up = y[SLOT:PART]
        h = jnp.where(keep, gate / (1.0 + jnp.exp(-gate)) * up, 0.0).astype(BF16)
        for k in range(4):
            out_ref[j, k] = h


def hidden_of(received, gate_scale, up_scale):
    vm = pl.BlockSpec(memory_space=pltpu.VMEM)
    return pl.pallas_call(
        hidden_kernel,
        in_specs=[vm, vm, vm],
        out_specs=[vm, vm],
        out_shape=[pltpu.VMEM((4, 4, SLOT, CHUNK), BF16), pltpu.VMEM((8, ROWS), F32)],
        name="hidden",
    )(*[near(a) for a in (received, gate_scale, up_scale)])


def down_kernel(h_ref, w0_ref, w1_ref, w2_ref, w3_ref, out_ref):
    me = lax.axis_index("zl") * 2 + lax.axis_index("yl")
    row = iota((FFL, 4 * SLOT), 0)
    lane = iota((FFL, 4 * SLOT), 1)
    hit = lane < 0
    for k in range(4):
        hit = hit | ((lane == row + (SLOT - UNITS) * k) & (row >= UNITS * k) & (row < UNITS * (k + 1)))
    squeeze = one_hot(hit)
    acc = jnp.zeros((CHUNK, COLS), F32)
    for r, w_ref in enumerate((w0_ref, w1_ref, w2_ref, w3_ref)):
        h = dot(h_ref[me ^ r], squeeze, 0, 1).astype(BF16)
        acc = acc + dot(h, w_ref[...], 1, 0)
    out_ref[...] = acc.astype(BF16)


def down(hidden, weights):
    vm = pl.BlockSpec(memory_space=pltpu.VMEM)
    return pl.pallas_call(
        down_kernel,
        in_specs=[vm] * 5,
        out_specs=vm,
        out_shape=pltpu.VMEM((CHUNK, COLS), BF16),
        name="down",
    )(near(hidden), *[near(w) for w in weights])


def mix_kernel(r_ref, x_ref, stat_ref, gain_ref, bias_ref, scale_ref, mixed_ref, part_ref):
    member = lax.axis_index("zl") * 2 + lax.axis_index("yl")
    at = member * CHUNK + (lax.axis_index("Z") * 4 + lax.axis_index("Y")) * 16
    branch = jnp.zeros((16, COLS), F32)
    for k in range(16):
        branch = branch + r_ref[k].astype(F32)
    mine = iota((16, ROWS), 1) == iota((16, ROWS), 0) + at
    mean = jnp.sum(jnp.where(mine, stat_ref[0:1], 0.0), axis=1, keepdims=True)
    rstd = jnp.sum(jnp.where(mine, stat_ref[1:2], 0.0), axis=1, keepdims=True)
    normed = rounded((x_ref[...].astype(F32) - mean) * rstd * gain_ref[...] + bias_ref[...])
    mixed = 0.5 * normed + branch * scale_ref[...]
    mixed_ref[...] = mixed
    m = jnp.sum(mixed, axis=1, keepdims=True) * (1.0 / COLS)
    c = mixed - m
    m2 = jnp.sum(c * c, axis=1, keepdims=True)
    lane = iota((16, 128), 1)
    part = jnp.where(lane == 0, m, jnp.where(lane == 1, m2, 0.0))
    for k in range(4):
        part_ref[k] = part


def mix(received, own, stats, gain, bias, scale):
    vm = pl.BlockSpec(memory_space=pltpu.VMEM)
    return pl.pallas_call(
        mix_kernel,
        in_specs=[vm] * 6,
        out_specs=[vm, vm],
        out_shape=[pltpu.VMEM((16, COLS), F32), pltpu.VMEM((4, 16, 128), F32)],
        name="mix",
    )(*[near(a) for a in (received, own, stats, gain, bias, scale)])


def finish_kernel(mixed_ref, part_ref, gain_ref, bias_ref, out_ref):
    parts = [part_ref[k] for k in range(4)]
    means = [p[:, 0:1] for p in parts]
    mean = (means[0] + means[1] + means[2] + means[3]) * 0.25
    m2 = sum(p[:, 1:2] for p in parts) + COLS * sum((v - mean) * (v - mean) for v in means)
    rstd = lax.rsqrt(m2 * (1.0 / D) + 1e-05)
    out_ref[...] = ((mixed_ref[...] - mean) * rstd * gain_ref[...] + bias_ref[...]).astype(BF16)


def finish(mixed, parts, gain, bias):
    vm = pl.BlockSpec(memory_space=pltpu.VMEM)
    return pl.pallas_call(
        finish_kernel,
        in_specs=[vm] * 4,
        out_specs=vm,
        out_shape=jax.ShapeDtypeStruct((16, COLS), BF16),
        name="finish",
    )(*[near(a) for a in (mixed, parts, gain, bias)])


def swapped(n, k):
    return [(i, i ^ k) for i in range(n)]


def local(
    tokens,
    norm_gain,
    norm_bias,
    gate_weight,
    up_weight,
    gate_scale,
    up_scale,
    down_weight,
    down_scale,
    out_gain,
    out_bias,
):
    gain = norm_gain.reshape(1, COLS)
    bias = norm_bias.reshape(1, COLS)

    w0 = down_weight.astype(BF16)
    w1 = lax.ppermute(w0, "yl", swapped(2, 1))
    w2 = lax.ppermute(w0, "zl", swapped(2, 1))
    w3 = lax.ppermute(w0, ("zl", "yl"), swapped(4, 3))

    shares = project(tokens, gate_weight.T, up_weight.T, gain, bias)
    received = lax.all_to_all(shares, "cb", 0, 0, tiled=True)
    sent, stats = hidden_of(received, gate_scale.reshape(1, FFL), up_scale.reshape(1, FFL))
    hidden = lax.all_to_all(sent.reshape(16, SLOT, CHUNK), ("zl", "yl", "cb"), 0, 0, tiled=True)
    own = lax.dynamic_slice_in_dim(tokens, lax.axis_index(RA) * 16, 16, 0)
    hidden, own = lax.optimization_barrier((hidden, own))
    partial = down(hidden.reshape(4, 4 * SLOT, CHUNK), (w0, w1, w2, w3))
    pieces = lax.all_to_all(partial.reshape(16, 16, COLS), ("Z", "Y"), 0, 0, tiled=True)
    mixed, part = mix(pieces, own, stats, gain, bias, down_scale.reshape(1, COLS))
    parts = lax.all_to_all(part, "cb", 0, 0, tiled=True)
    return finish(mixed, parts, out_gain.reshape(1, COLS), out_bias.reshape(1, COLS))


def solution(mesh):
    split = Mesh(mesh.devices.reshape(4, 2, 4, 2, 4, 2), RA + ("cb", "dp"))
    return jax.shard_map(
        local,
        mesh=split,
        in_specs=(
            P("dp", "cb"),
            P("cb"),
            P("cb"),
            P("cb", RA),
            P("cb", RA),
            P(RA),
            P(RA),
            P(RA, "cb"),
            P("cb"),
            P("cb"),
            P("cb"),
        ),
        out_specs=P(("dp",) + RA, "cb"),
        check_vma=False,
    )
```

```python
import jax
import jax.numpy as jnp
from jax import lax
from jax.experimental import pallas as pl
from jax.experimental.pallas import tpu as pltpu
from jax.sharding import Mesh, PartitionSpec as P


D = 4096
F32 = jnp.float32
BF16 = jnp.bfloat16
RA = ("Z", "zl", "Y", "yl")
UNITS = 44
SLOT = 48
PART = 2 * SLOT
ROWS = 1024
COLS = 1024
FFL = 176
CHUNK = 256


def iota(shape, dim):
    return lax.broadcasted_iota(jnp.int32, shape, dim)


def near(a):
    return pltpu.with_memory_space_constraint(a, pltpu.VMEM)


def dot(a, b, ca, cb):
    return lax.dot_general(a, b, (((ca,), (cb,)), ((), ())), preferred_element_type=F32)


def rounded(v):
    return v.astype(BF16).astype(F32)


def one_hot(cond):
    return jnp.where(cond, 1.0, 0.0).astype(BF16)


def project_kernel(x_ref, gw_ref, uw_ref, gain_ref, bias_ref, out_ref, x_buf, gw_buf, uw_buf, gb_buf, out_buf, w_ref, vec_ref, sems):
    loads = [
        pltpu.make_async_copy(gw_ref, gw_buf, sems.at[0]),
        pltpu.make_async_copy(uw_ref, uw_buf, sems.at[1]),
        pltpu.make_async_copy(gain_ref, gb_buf.at[0], sems.at[2]),
        pltpu.make_async_copy(bias_ref, gb_buf.at[1], sems.at[3]),
    ]
    tokens = [pltpu.make_async_copy(x_ref.at[:, j // 2, :, j % 2], x_buf.at[j], sems.at[4 + j]) for j in range(4)]
    for copy in loads + tokens[:1]:
        copy.start()
    for copy in loads:
        copy.wait()
    for copy in tokens[1:]:
        copy.start()

    gain = gb_buf[0]
    row = iota((SLOT, COLS), 0)
    for k in range(4):
        first = UNITS * k - 4 * (k % 2)
        for half, ref in enumerate((gw_buf, uw_buf)):
            w = ref[first : min(first + SLOT + 8 * (k % 2), FFL)] * gain
            if k % 2:
                w = pltpu.roll(w, w.shape[0] - 4, 0)
            fill = jnp.where(row == UNITS, 1.0, 0.0) if half == 0 else 0.0
            at = PART * k + SLOT * half
            w_ref[at : at + SLOT, :] = jnp.where(row < UNITS, w[0:SLOT], fill).astype(BF16)
    r = iota((128, COLS), 0)
    ratio = gb_buf[1] / gain
    rh = rounded(ratio)
    lead = jnp.where(r == 0, 1.0, jnp.where(r == 1, rh, jnp.where(r == 2, ratio - rh, 0.0))).astype(BF16)
    cols = dot(w_ref[...], lead, 1, 1)
    col = cols[:, 0:1]
    sums = cols.T
    both = jnp.concatenate([sums[0:1], sums[1:2] + sums[2:3], jnp.zeros((1, ROWS - 8 * PART), F32)], axis=1)
    hi = rounded(both)
    q = iota((8, ROWS), 0)
    vec_ref[...] = jnp.where(q == 0, hi, jnp.where(q == 1, both - hi, 0.0))

    stores = []
    for j in range(4):
        at = slice(CHUNK * j, CHUNK * (j + 1))
        tokens[j].wait()
        part = dot(w_ref[...], x_buf[j].reshape(CHUNK, COLS), 1, 1)
        x = x_buf[j].reshape(CHUNK, COLS).astype(F32)
        pivot = x[:, 0:1]
        c = x - pivot
        sq = jnp.sum(c * c, axis=1, keepdims=True)
        lane = iota((CHUNK, 128), 1)
        stat = jnp.where(lane == 0, sq, jnp.where(lane == 1, pivot, 0.0)).T
        m_row = part[UNITS : UNITS + 1] * (1.0 / COLS)
        off = m_row - stat[1:2]
        m2_row = stat[0:1] - COLS * off * off
        m_hi = rounded(m_row)
        m_mid = rounded(m_row - m_hi)
        m_lo = m_row - m_hi - m_mid
        m2_hi = rounded(m2_row)
        m2_lo = m2_row - m2_hi
        r = iota((8, CHUNK), 0)
        t1 = jnp.where(r == 4, m_hi, jnp.where(r == 5, m_mid, jnp.where(r == 6, m_lo, jnp.where(r == 7, vec_ref[0:1, at], 0.0))))
        t2 = jnp.where(r == 4, m2_hi, jnp.where(r == 5, m2_lo, jnp.where(r == 6, vec_ref[1:2, at], 0.0)))
        z = jnp.zeros((SLOT - 8, CHUNK), F32)
        extra = jnp.concatenate([z, t1, z, t2], axis=0)
        for k in range(4):
            rows = slice(PART * k, PART * (k + 1))
            out_buf[k, :, at] = (part[rows] - col[rows] * m_row + extra).astype(BF16)
        stores.append(pltpu.make_async_copy(out_buf.at[:, :, at], out_ref.at[:, :, at], sems.at[8 + j]))
        stores[-1].start()
    for copy in stores:
        copy.wait()


def project(tokens, gate_t, up_t, gain, bias):
    hbm = pl.BlockSpec(memory_space=pl.ANY)
    return pl.pallas_call(
        project_kernel,
        in_specs=[hbm] * 5,
        out_specs=hbm,
        out_shape=pltpu.HBM((4, PART, ROWS), BF16),
        scratch_shapes=[
            pltpu.VMEM((4, 4, 4, 16, COLS), BF16),
            pltpu.VMEM((FFL, COLS), F32),
            pltpu.VMEM((FFL, COLS), F32),
            pltpu.VMEM((2, 1, COLS), F32),
            pltpu.VMEM((4, PART, ROWS), BF16),
            pltpu.VMEM((4 * PART, COLS), BF16),
            pltpu.VMEM((8, ROWS), F32),
            pltpu.SemaphoreType.DMA((12,)),
        ],
        name="project",
    )(*[pltpu.with_memory_space_constraint(a, pltpu.HBM) for a in (tokens.reshape(4, 2, 4, 2, 16, COLS), gate_t, up_t, gain, bias)])


def hidden_kernel(r_ref, gs_ref, us_ref, out_ref, stat_ref):
    me = lax.axis_index("cb")
    means = []
    m2s = []
    for c in range(4):
        a = r_ref[c, 32:48, :].astype(F32)
        b = r_ref[c, 80:96, :].astype(F32)
        means.append(a[12:13] + a[13:14] + a[14:15])
        m2s.append(b[12:13] + b[13:14])
    mean = (means[0] + means[1] + means[2] + means[3]) * 0.25
    deltas = [v - mean for v in means]
    m2 = sum(m2s) + COLS * sum(d * d for d in deltas)
    rstd = lax.rsqrt(m2 * (1.0 / D) + 1e-05)
    q = iota((8, ROWS), 0)
    stat_ref[...] = jnp.where(q == 0, mean, jnp.where(q == 1, rstd, 0.0))

    wide = 8 * PART
    pick_row = iota((2 * PART, wide), 0)
    pick_lane = iota((2 * PART, wide), 1)
    base = jnp.where(pick_row < PART, me * PART, (4 + me) * PART - PART)
    pick = one_hot(pick_lane == pick_row + base)
    tiles = [r_ref[c, 32:48, 0:wide] for c in range(4)] + [r_ref[c, 80:96, 0:wide] for c in range(4)]
    vecs = dot(pick, jnp.concatenate(tiles, axis=0), 1, 1)
    col_sums = [vecs[0:PART, 16 * c + 15 : 16 * c + 16] + vecs[0:PART, 78 + 16 * c : 79 + 16 * c] for c in range(4)]
    biases = sum(vecs[PART:, 16 * c + 15 : 16 * c + 16] + vecs[PART:, 78 + 16 * c : 79 + 16 * c] for c in range(4))

    gs = gs_ref[...]
    us = us_ref[...]
    g1 = rounded(gs)
    g2 = rounded(gs - g1)
    u1 = rounded(us)
    u2 = rounded(us - u1)
    sr = iota((16, FFL), 0)
    pieces = jnp.where(sr == 0, g1, jnp.where(sr == 1, g2, jnp.where(sr == 2, gs - g1 - g2, 0.0)))
    pieces = pieces + jnp.where(sr == 3, u1, jnp.where(sr == 4, u2, jnp.where(sr == 5, us - u1 - u2, 0.0)))
    row = iota((PART, FFL), 0)
    unit = jnp.where(row < SLOT, row, row - SLOT)
    own = one_hot((iota((PART, FFL), 1) == unit + me * UNITS) & (unit < UNITS))
    sc = dot(own, pieces.astype(BF16), 1, 1)
    scale = jnp.where(iota((PART, 1), 0) < SLOT, sc[:, 0:1] + sc[:, 1:2] + sc[:, 2:3], sc[:, 3:4] + sc[:, 4:5] + sc[:, 5:6])

    keep = iota((SLOT, CHUNK), 0) < UNITS
    for j in range(4):
        at = slice(CHUNK * j, CHUNK * (j + 1))
        acc = jnp.zeros((PART, CHUNK), F32)
        for c in range(4):
            acc = acc + (r_ref[c, :, at].astype(F32) + col_sums[c] * deltas[c][:, at])
        y = (acc * rstd[:, at] + biases) * scale
        gate = y[0:SLOT]
        up = y[SLOT:PART]
        h = jnp.where(keep, gate / (1.0 + jnp.exp(-gate)) * up, 0.0).astype(BF16)
        for k in range(4):
            out_ref[j, k] = h


def hidden_of(received, gate_scale, up_scale):
    vm = pl.BlockSpec(memory_space=pltpu.VMEM)
    return pl.pallas_call(
        hidden_kernel,
        in_specs=[vm, vm, vm],
        out_specs=[vm, vm],
        out_shape=[pltpu.VMEM((4, 4, SLOT, CHUNK), BF16), pltpu.VMEM((8, ROWS), F32)],
        name="hidden",
    )(*[near(a) for a in (received, gate_scale, up_scale)])


def down_kernel(h_ref, own_ref, fetched_ref, other_ref, out_ref):
    me = lax.axis_index("zl") * 2 + lax.axis_index("yl")
    core = lax.axis_index("dp")

    def squeezed(member, first, count):
        unit = iota((count, 4 * SLOT), 0) + first
        lane = iota((count, 4 * SLOT), 1)
        hit = lane < 0
        for k in range(4):
            hit = hit | ((lane == unit + (SLOT - UNITS) * k) & (unit >= UNITS * k) & (unit < UNITS * (k + 1)))
        return dot(h_ref[member], one_hot(hit), 0, 1).astype(BF16)

    half = FFL // 2
    acc = dot(squeezed(me, 0, FFL), own_ref[...], 1, 0)
    acc = acc + dot(squeezed(me ^ (1 + core), 0, FFL), fetched_ref[0:FFL], 1, 0)
    acc = acc + dot(squeezed(me ^ (2 - core), 0, FFL), other_ref[0:FFL], 1, 0)
    acc = acc + dot(squeezed(me ^ 3, core * half, half), fetched_ref[FFL:], 1, 0)
    acc = acc + dot(squeezed(me ^ 3, half - core * half, half), other_ref[FFL:], 1, 0)
    out_ref[...] = acc.astype(BF16)


def down(hidden, weights):
    vm = pl.BlockSpec(memory_space=pltpu.VMEM)
    return pl.pallas_call(
        down_kernel,
        in_specs=[vm] * 4,
        out_specs=vm,
        out_shape=pltpu.VMEM((CHUNK, COLS), BF16),
        name="down",
    )(near(hidden), *[near(w) for w in weights])


def mix_kernel(r_ref, x_ref, stat_ref, gain_ref, bias_ref, scale_ref, mixed_ref, part_ref):
    member = lax.axis_index("zl") * 2 + lax.axis_index("yl")
    at = member * CHUNK + (lax.axis_index("Z") * 4 + lax.axis_index("Y")) * 16
    branch = jnp.zeros((16, COLS), F32)
    for k in range(16):
        branch = branch + r_ref[k].astype(F32)
    mine = iota((16, ROWS), 1) == iota((16, ROWS), 0) + at
    mean = jnp.sum(jnp.where(mine, stat_ref[0:1], 0.0), axis=1, keepdims=True)
    rstd = jnp.sum(jnp.where(mine, stat_ref[1:2], 0.0), axis=1, keepdims=True)
    normed = rounded((x_ref[...].astype(F32) - mean) * rstd * gain_ref[...] + bias_ref[...])
    mixed = 0.5 * normed + branch * scale_ref[...]
    mixed_ref[...] = mixed
    m = jnp.sum(mixed, axis=1, keepdims=True) * (1.0 / COLS)
    c = mixed - m
    m2 = jnp.sum(c * c, axis=1, keepdims=True)
    lane = iota((16, 128), 1)
    part = jnp.where(lane == 0, m, jnp.where(lane == 1, m2, 0.0))
    for k in range(4):
        part_ref[k] = part


def mix(received, own, stats, gain, bias, scale):
    vm = pl.BlockSpec(memory_space=pltpu.VMEM)
    return pl.pallas_call(
        mix_kernel,
        in_specs=[vm] * 6,
        out_specs=[vm, vm],
        out_shape=[pltpu.VMEM((16, COLS), F32), pltpu.VMEM((4, 16, 128), F32)],
        name="mix",
    )(*[near(a) for a in (received, own, stats, gain, bias, scale)])


def finish_kernel(mixed_ref, part_ref, gain_ref, bias_ref, out_ref):
    parts = [part_ref[k] for k in range(4)]
    means = [p[:, 0:1] for p in parts]
    mean = (means[0] + means[1] + means[2] + means[3]) * 0.25
    m2 = sum(p[:, 1:2] for p in parts) + COLS * sum((v - mean) * (v - mean) for v in means)
    rstd = lax.rsqrt(m2 * (1.0 / D) + 1e-05)
    out_ref[...] = ((mixed_ref[...] - mean) * rstd * gain_ref[...] + bias_ref[...]).astype(BF16)


def finish(mixed, parts, gain, bias):
    vm = pl.BlockSpec(memory_space=pltpu.VMEM)
    return pl.pallas_call(
        finish_kernel,
        in_specs=[vm] * 4,
        out_specs=vm,
        out_shape=jax.ShapeDtypeStruct((16, COLS), BF16),
        name="finish",
    )(*[near(a) for a in (mixed, parts, gain, bias)])


def swapped(n, k):
    return [(i, i ^ k) for i in range(n)]


def local(
    tokens,
    norm_gain,
    norm_bias,
    gate_weight,
    up_weight,
    gate_scale,
    up_scale,
    down_weight,
    down_scale,
    out_gain,
    out_bias,
):
    gain = norm_gain.reshape(1, COLS)
    bias = norm_bias.reshape(1, COLS)

    w0 = down_weight.astype(BF16)
    beside = lax.ppermute(w0, ("zl", "yl", "dp"), [(i, i ^ (4 if i & 1 else 2)) for i in range(8)])
    half = lax.dynamic_slice_in_dim(w0, lax.axis_index("dp") * (FFL // 2), FFL // 2, 0)
    across = lax.ppermute(half, ("zl", "yl"), swapped(4, 3))

    shares = project(tokens, gate_weight.T, up_weight.T, gain, bias)
    received = lax.all_to_all(shares, "cb", 0, 0, tiled=True)
    sent, stats = hidden_of(received, gate_scale.reshape(1, FFL), up_scale.reshape(1, FFL))
    hidden = lax.all_to_all(sent.reshape(16, SLOT, CHUNK), ("zl", "yl", "cb"), 0, 0, tiled=True)
    fetched = jnp.concatenate([beside, across], axis=0)
    other = lax.ppermute(fetched, "dp", swapped(2, 1))
    own = lax.dynamic_slice_in_dim(tokens, lax.axis_index(RA) * 16, 16, 0)
    hidden, own = lax.optimization_barrier((hidden, own))
    partial = down(hidden.reshape(4, 4 * SLOT, CHUNK), (w0, fetched, other))
    pieces = lax.all_to_all(partial.reshape(16, 16, COLS), ("Z", "Y"), 0, 0, tiled=True)
    mixed, part = mix(pieces, own, stats, gain, bias, down_scale.reshape(1, COLS))
    parts = lax.all_to_all(part, "cb", 0, 0, tiled=True)
    return finish(mixed, parts, out_gain.reshape(1, COLS), out_bias.reshape(1, COLS))


def solution(mesh):
    split = Mesh(mesh.devices.reshape(4, 2, 4, 2, 4, 2), RA + ("cb", "dp"))
    return jax.shard_map(
        local,
        mesh=split,
        in_specs=(
            P("dp", "cb"),
            P("cb"),
            P("cb"),
            P("cb", RA),
            P("cb", RA),
            P(RA),
            P(RA),
            P(RA, "cb"),
            P("cb"),
            P("cb"),
            P("cb"),
        ),
        out_specs=P(("dp",) + RA, "cb"),
        check_vma=False,
    )
```

```python
import jax
import jax.numpy as jnp
from jax import lax
from jax.experimental import pallas as pl
from jax.experimental.pallas import tpu as pltpu
from jax.sharding import Mesh, PartitionSpec as P


D = 4096
F32 = jnp.float32
BF16 = jnp.bfloat16
RA = ("Z", "zl", "Y", "yl")
UNITS = 44
SLOT = 48
PART = 2 * SLOT
ROWS = 1024
COLS = 1024
FFL = 176
CHUNK = 256
PER = 2
TILE = PER * CHUNK


def iota(shape, dim):
    return lax.broadcasted_iota(jnp.int32, shape, dim)


def near(a):
    return pltpu.with_memory_space_constraint(a, pltpu.VMEM)


def dot(a, b, ca, cb):
    return lax.dot_general(a, b, (((ca,), (cb,)), ((), ())), preferred_element_type=F32)


def rounded(v):
    return v.astype(BF16).astype(F32)


def one_hot(cond):
    return jnp.where(cond, 1.0, 0.0).astype(BF16)


def project_kernel(x_ref, gw_ref, uw_ref, gain_ref, bias_ref, out_ref, x_buf, gw_buf, uw_buf, gb_buf, out_buf, w_ref, vec_ref, sems):
    loads = [
        pltpu.make_async_copy(gw_ref, gw_buf, sems.at[0]),
        pltpu.make_async_copy(uw_ref, uw_buf, sems.at[1]),
        pltpu.make_async_copy(gain_ref, gb_buf.at[0], sems.at[2]),
        pltpu.make_async_copy(bias_ref, gb_buf.at[1], sems.at[3]),
    ]
    tokens = [pltpu.make_async_copy(x_ref.at[:, j // 2, :, j % 2], x_buf.at[j], sems.at[4 + j]) for j in range(4)]
    for copy in loads + tokens[:PER]:
        copy.start()
    for copy in loads:
        copy.wait()
    for copy in tokens[PER:]:
        copy.start()

    gain = gb_buf[0]
    row = iota((SLOT, COLS), 0)
    for k in range(4):
        first = UNITS * k - 4 * (k % 2)
        for half, ref in enumerate((gw_buf, uw_buf)):
            w = ref[first : min(first + SLOT + 8 * (k % 2), FFL)] * gain
            if k % 2:
                w = pltpu.roll(w, w.shape[0] - 4, 0)
            fill = jnp.where(row == UNITS, 1.0, 0.0) if half == 0 else 0.0
            at = PART * k + SLOT * half
            w_ref[at : at + SLOT, :] = jnp.where(row < UNITS, w[0:SLOT], fill).astype(BF16)
    r = iota((128, COLS), 0)
    ratio = gb_buf[1] / gain
    rh = rounded(ratio)
    lead = jnp.where(r == 0, 1.0, jnp.where(r == 1, rh, jnp.where(r == 2, ratio - rh, 0.0))).astype(BF16)
    cols = dot(w_ref[...], lead, 1, 1)
    col = cols[:, 0:1]
    sums = cols.T
    both = jnp.concatenate([sums[0:1], sums[1:2] + sums[2:3], jnp.zeros((1, ROWS - 8 * PART), F32)], axis=1)
    hi = rounded(both)
    q = iota((8, ROWS), 0)
    vec_ref[...] = jnp.where(q == 0, hi, jnp.where(q == 1, both - hi, 0.0))

    stores = []
    for j in range(4 // PER):
        at = slice(TILE * j, TILE * (j + 1))
        for copy in tokens[PER * j : PER * (j + 1)]:
            copy.wait()
        part = dot(w_ref[...], x_buf[PER * j : PER * (j + 1)].reshape(TILE, COLS), 1, 1)
        x = x_buf[PER * j : PER * (j + 1)].reshape(TILE, COLS).astype(F32)
        pivot = x[:, 0:1]
        c = x - pivot
        sq = jnp.sum(c * c, axis=1, keepdims=True)
        lane = iota((TILE, 128), 1)
        stat = jnp.where(lane == 0, sq, jnp.where(lane == 1, pivot, 0.0)).T
        m_row = part[UNITS : UNITS + 1] * (1.0 / COLS)
        off = m_row - stat[1:2]
        m2_row = stat[0:1] - COLS * off * off
        m_hi = rounded(m_row)
        m_mid = rounded(m_row - m_hi)
        m_lo = m_row - m_hi - m_mid
        m2_hi = rounded(m2_row)
        m2_lo = m2_row - m2_hi
        r = iota((8, TILE), 0)
        t1 = jnp.where(r == 4, m_hi, jnp.where(r == 5, m_mid, jnp.where(r == 6, m_lo, jnp.where(r == 7, vec_ref[0:1, at], 0.0))))
        t2 = jnp.where(r == 4, m2_hi, jnp.where(r == 5, m2_lo, jnp.where(r == 6, vec_ref[1:2, at], 0.0)))
        z = jnp.zeros((SLOT - 8, TILE), F32)
        extra = jnp.concatenate([z, t1, z, t2], axis=0)
        for k in range(4):
            rows = slice(PART * k, PART * (k + 1))
            out_buf[k, :, at] = (part[rows] - col[rows] * m_row + extra).astype(BF16)
        stores.append(pltpu.make_async_copy(out_buf.at[:, :, at], out_ref.at[:, :, at], sems.at[8 + j]))
        stores[-1].start()
    for copy in stores:
        copy.wait()


def project(tokens, gate_t, up_t, gain, bias):
    hbm = pl.BlockSpec(memory_space=pl.ANY)
    return pl.pallas_call(
        project_kernel,
        in_specs=[hbm] * 5,
        out_specs=hbm,
        out_shape=pltpu.HBM((4, PART, ROWS), BF16),
        scratch_shapes=[
            pltpu.VMEM((4, 4, 4, 16, COLS), BF16),
            pltpu.VMEM((FFL, COLS), F32),
            pltpu.VMEM((FFL, COLS), F32),
            pltpu.VMEM((2, 1, COLS), F32),
            pltpu.VMEM((4, PART, ROWS), BF16),
            pltpu.VMEM((4 * PART, COLS), BF16),
            pltpu.VMEM((8, ROWS), F32),
            pltpu.SemaphoreType.DMA((12,)),
        ],
        name="project",
    )(*[pltpu.with_memory_space_constraint(a, pltpu.HBM) for a in (tokens.reshape(4, 2, 4, 2, 16, COLS), gate_t, up_t, gain, bias)])


def hidden_kernel(r_ref, gs_ref, us_ref, out_ref, stat_ref):
    me = lax.axis_index("cb")
    means = []
    m2s = []
    for c in range(4):
        a = r_ref[c, 32:48, :].astype(F32)
        b = r_ref[c, 80:96, :].astype(F32)
        means.append(a[12:13] + a[13:14] + a[14:15])
        m2s.append(b[12:13] + b[13:14])
    mean = (means[0] + means[1] + means[2] + means[3]) * 0.25
    deltas = [v - mean for v in means]
    m2 = sum(m2s) + COLS * sum(d * d for d in deltas)
    rstd = lax.rsqrt(m2 * (1.0 / D) + 1e-05)
    q = iota((8, ROWS), 0)
    stat_ref[...] = jnp.where(q == 0, mean, jnp.where(q == 1, rstd, 0.0))

    wide = 8 * PART
    pick_row = iota((2 * PART, wide), 0)
    pick_lane = iota((2 * PART, wide), 1)
    base = jnp.where(pick_row < PART, me * PART, (4 + me) * PART - PART)
    pick = one_hot(pick_lane == pick_row + base)
    tiles = [r_ref[c, 32:48, 0:wide] for c in range(4)] + [r_ref[c, 80:96, 0:wide] for c in range(4)]
    vecs = dot(pick, jnp.concatenate(tiles, axis=0), 1, 1)
    col_sums = [vecs[0:PART, 16 * c + 15 : 16 * c + 16] + vecs[0:PART, 78 + 16 * c : 79 + 16 * c] for c in range(4)]
    biases = sum(vecs[PART:, 16 * c + 15 : 16 * c + 16] + vecs[PART:, 78 + 16 * c : 79 + 16 * c] for c in range(4))

    gs = gs_ref[...]
    us = us_ref[...]
    g1 = rounded(gs)
    g2 = rounded(gs - g1)
    u1 = rounded(us)
    u2 = rounded(us - u1)
    sr = iota((16, FFL), 0)
    pieces = jnp.where(sr == 0, g1, jnp.where(sr == 1, g2, jnp.where(sr == 2, gs - g1 - g2, 0.0)))
    pieces = pieces + jnp.where(sr == 3, u1, jnp.where(sr == 4, u2, jnp.where(sr == 5, us - u1 - u2, 0.0)))
    row = iota((PART, FFL), 0)
    unit = jnp.where(row < SLOT, row, row - SLOT)
    own = one_hot((iota((PART, FFL), 1) == unit + me * UNITS) & (unit < UNITS))
    sc = dot(own, pieces.astype(BF16), 1, 1)
    scale = jnp.where(iota((PART, 1), 0) < SLOT, sc[:, 0:1] + sc[:, 1:2] + sc[:, 2:3], sc[:, 3:4] + sc[:, 4:5] + sc[:, 5:6])

    keep = iota((SLOT, CHUNK), 0) < UNITS
    for j in range(4):
        at = slice(CHUNK * j, CHUNK * (j + 1))
        acc = jnp.zeros((PART, CHUNK), F32)
        for c in range(4):
            acc = acc + (r_ref[c, :, at].astype(F32) + col_sums[c] * deltas[c][:, at])
        y = (acc * rstd[:, at] + biases) * scale
        gate = y[0:SLOT]
        up = y[SLOT:PART]
        h = jnp.where(keep, gate / (1.0 + jnp.exp(-gate)) * up, 0.0).astype(BF16)
        for k in range(4):
            out_ref[j, k] = h


def hidden_of(received, gate_scale, up_scale):
    vm = pl.BlockSpec(memory_space=pltpu.VMEM)
    return pl.pallas_call(
        hidden_kernel,
        in_specs=[vm, vm, vm],
        out_specs=[vm, vm],
        out_shape=[pltpu.VMEM((4, 4, SLOT, CHUNK), BF16), pltpu.VMEM((8, ROWS), F32)],
        name="hidden",
    )(*[near(a) for a in (received, gate_scale, up_scale)])


def down_kernel(h_ref, own_ref, fetched_ref, other_ref, out_ref):
    me = lax.axis_index("zl") * 2 + lax.axis_index("yl")
    core = lax.axis_index("dp")

    unit = iota((FFL, 4 * SLOT), 0)
    slot = jnp.where(unit < 2 * UNITS, jnp.where(unit < UNITS, 0, 1), jnp.where(unit < 3 * UNITS, 2, 3))
    place = one_hot(iota((FFL, 4 * SLOT), 1) == unit + (SLOT - UNITS) * slot)

    def squeezed(member):
        return dot(h_ref[member], place, 0, 1).astype(BF16)

    acc = dot(squeezed(me), own_ref[...], 1, 0)
    acc = acc + dot(squeezed(me ^ (1 + core)), fetched_ref[:, 0:COLS], 1, 0)
    acc = acc + dot(squeezed(me ^ (2 - core)), other_ref[:, 0:COLS], 1, 0)
    h = squeezed(me ^ 3)
    mine = dot(h, fetched_ref[:, COLS:], 1, 0)
    theirs = dot(h, other_ref[:, COLS:], 1, 0)
    acc = acc + jnp.concatenate([jnp.where(core == 0, mine, theirs), jnp.where(core == 0, theirs, mine)], axis=1)
    out_ref[...] = acc.astype(BF16)


def down(hidden, weights):
    vm = pl.BlockSpec(memory_space=pltpu.VMEM)
    return pl.pallas_call(
        down_kernel,
        in_specs=[vm] * 4,
        out_specs=vm,
        out_shape=pltpu.VMEM((CHUNK, COLS), BF16),
        name="down",
    )(near(hidden), *[near(w) for w in weights])


def mix_kernel(r_ref, x_ref, stat_ref, gain_ref, bias_ref, scale_ref, mixed_ref, part_ref):
    member = lax.axis_index("zl") * 2 + lax.axis_index("yl")
    at = member * CHUNK + (lax.axis_index("Z") * 4 + lax.axis_index("Y")) * 16
    branch = jnp.zeros((16, COLS), F32)
    for k in range(16):
        branch = branch + r_ref[k].astype(F32)
    mine = iota((16, ROWS), 1) == iota((16, ROWS), 0) + at
    mean = jnp.sum(jnp.where(mine, stat_ref[0:1], 0.0), axis=1, keepdims=True)
    rstd = jnp.sum(jnp.where(mine, stat_ref[1:2], 0.0), axis=1, keepdims=True)
    normed = rounded((x_ref[...].astype(F32) - mean) * rstd * gain_ref[...] + bias_ref[...])
    mixed = 0.5 * normed + branch * scale_ref[...]
    mixed_ref[...] = mixed
    m = jnp.sum(mixed, axis=1, keepdims=True) * (1.0 / COLS)
    c = mixed - m
    m2 = jnp.sum(c * c, axis=1, keepdims=True)
    lane = iota((16, 128), 1)
    part = jnp.where(lane == 0, m, jnp.where(lane == 1, m2, 0.0))
    for k in range(4):
        part_ref[k] = part


def mix(received, own, stats, gain, bias, scale):
    vm = pl.BlockSpec(memory_space=pltpu.VMEM)
    return pl.pallas_call(
        mix_kernel,
        in_specs=[vm] * 6,
        out_specs=[vm, vm],
        out_shape=[pltpu.VMEM((16, COLS), F32), pltpu.VMEM((4, 16, 128), F32)],
        name="mix",
    )(*[near(a) for a in (received, own, stats, gain, bias, scale)])


def finish_kernel(mixed_ref, part_ref, gain_ref, bias_ref, out_ref):
    parts = [part_ref[k] for k in range(4)]
    means = [p[:, 0:1] for p in parts]
    mean = (means[0] + means[1] + means[2] + means[3]) * 0.25
    m2 = sum(p[:, 1:2] for p in parts) + COLS * sum((v - mean) * (v - mean) for v in means)
    rstd = lax.rsqrt(m2 * (1.0 / D) + 1e-05)
    out_ref[...] = ((mixed_ref[...] - mean) * rstd * gain_ref[...] + bias_ref[...]).astype(BF16)


def finish(mixed, parts, gain, bias):
    vm = pl.BlockSpec(memory_space=pltpu.VMEM)
    return pl.pallas_call(
        finish_kernel,
        in_specs=[vm] * 4,
        out_specs=vm,
        out_shape=jax.ShapeDtypeStruct((16, COLS), BF16),
        name="finish",
    )(*[near(a) for a in (mixed, parts, gain, bias)])


def swapped(n, k):
    return [(i, i ^ k) for i in range(n)]


def local(
    tokens,
    norm_gain,
    norm_bias,
    gate_weight,
    up_weight,
    gate_scale,
    up_scale,
    down_weight,
    down_scale,
    out_gain,
    out_bias,
):
    gain = norm_gain.reshape(1, COLS)
    bias = norm_bias.reshape(1, COLS)

    w0 = down_weight.astype(BF16)
    beside = lax.ppermute(w0, ("zl", "yl", "dp"), [(i, i ^ (4 if i & 1 else 2)) for i in range(8)])
    half = lax.dynamic_slice_in_dim(w0, lax.axis_index("dp") * (COLS // 2), COLS // 2, 1)
    across = lax.ppermute(half, ("zl", "yl"), swapped(4, 3))

    shares = project(tokens, gate_weight.T, up_weight.T, gain, bias)
    received = lax.all_to_all(shares, "cb", 0, 0, tiled=True)
    sent, stats = hidden_of(received, gate_scale.reshape(1, FFL), up_scale.reshape(1, FFL))
    own = lax.dynamic_slice_in_dim(tokens, lax.axis_index(RA) * 16, 16, 0)
    sent, own = lax.optimization_barrier((sent, own))
    hidden = lax.all_to_all(sent.reshape(16, SLOT, CHUNK), ("zl", "yl", "cb"), 0, 0, tiled=True)
    fetched = jnp.concatenate([beside, across], axis=1)
    other = lax.ppermute(fetched, "dp", swapped(2, 1))
    partial = down(hidden.reshape(4, 4 * SLOT, CHUNK), (w0, fetched, other))
    pieces = lax.all_to_all(partial.reshape(16, 16, COLS), ("Z", "Y"), 0, 0, tiled=True)
    mixed, part = mix(pieces, own, stats, gain, bias, down_scale.reshape(1, COLS))
    parts = lax.all_to_all(part, "cb", 0, 0, tiled=True)
    return finish(mixed, parts, out_gain.reshape(1, COLS), out_bias.reshape(1, COLS))


def solution(mesh):
    split = Mesh(mesh.devices.reshape(4, 2, 4, 2, 4, 2), RA + ("cb", "dp"))
    return jax.shard_map(
        local,
        mesh=split,
        in_specs=(
            P("dp", "cb"),
            P("cb"),
            P("cb"),
            P("cb", RA),
            P("cb", RA),
            P(RA),
            P(RA),
            P(RA, "cb"),
            P("cb"),
            P("cb"),
            P("cb"),
        ),
        out_specs=P(("dp",) + RA, "cb"),
        check_vma=False,
    )
```

```python
import jax
import jax.numpy as jnp
from jax import lax
from jax.experimental import pallas as pl
from jax.experimental.pallas import tpu as pltpu
from jax.sharding import Mesh, PartitionSpec as P


D = 4096
F32 = jnp.float32
BF16 = jnp.bfloat16
RA = ("Z", "zl", "Y", "yl")
UNITS = 44
SLOT = 48
PART = 2 * SLOT
ROWS = 1024
COLS = 1024
FFL = 176
CHUNK = 256
PER = 2
TILE = PER * CHUNK


def iota(shape, dim):
    return lax.broadcasted_iota(jnp.int32, shape, dim)


def near(a):
    return pltpu.with_memory_space_constraint(a, pltpu.VMEM)


def dot(a, b, ca, cb):
    return lax.dot_general(a, b, (((ca,), (cb,)), ((), ())), preferred_element_type=F32)


def rounded(v):
    return v.astype(BF16).astype(F32)


def one_hot(cond):
    return jnp.where(cond, 1.0, 0.0).astype(BF16)


def project_kernel(x_ref, gw_ref, uw_ref, gain_ref, bias_ref, out_ref, x_buf, gw_buf, uw_buf, gb_buf, out_buf, w_ref, vec_ref, sems):
    loads = [
        pltpu.make_async_copy(gw_ref, gw_buf, sems.at[0]),
        pltpu.make_async_copy(uw_ref, uw_buf, sems.at[1]),
        pltpu.make_async_copy(gain_ref, gb_buf.at[0], sems.at[2]),
        pltpu.make_async_copy(bias_ref, gb_buf.at[1], sems.at[3]),
    ]
    tokens = [pltpu.make_async_copy(x_ref.at[:, j // 2, :, j % 2], x_buf.at[j], sems.at[4 + j]) for j in range(4)]
    for copy in loads + tokens[:PER]:
        copy.start()
    for copy in loads:
        copy.wait()
    for copy in tokens[PER:]:
        copy.start()

    gain = gb_buf[0]
    row = iota((SLOT, COLS), 0)
    for k in range(4):
        first = UNITS * k - 4 * (k % 2)
        for half, ref in enumerate((gw_buf, uw_buf)):
            w = ref[first : min(first + SLOT + 8 * (k % 2), FFL)] * gain
            if k % 2:
                w = pltpu.roll(w, w.shape[0] - 4, 0)
            fill = jnp.where(row == UNITS, 1.0, 0.0) if half == 0 else 0.0
            at = PART * k + SLOT * half
            w_ref[at : at + SLOT, :] = jnp.where(row < UNITS, w[0:SLOT], fill).astype(BF16)
    r = iota((128, COLS), 0)
    ratio = gb_buf[1] / gain
    rh = rounded(ratio)
    lead = jnp.where(r == 0, 1.0, jnp.where(r == 1, rh, jnp.where(r == 2, ratio - rh, 0.0))).astype(BF16)
    cols = dot(w_ref[...], lead, 1, 1)
    col = cols[:, 0:1]
    sums = cols.T
    both = jnp.concatenate([sums[0:1], sums[1:2] + sums[2:3], jnp.zeros((1, ROWS - 8 * PART), F32)], axis=1)
    hi = rounded(both)
    q = iota((8, ROWS), 0)
    vec_ref[...] = jnp.where(q == 0, hi, jnp.where(q == 1, both - hi, 0.0))

    stores = []
    for j in range(4 // PER):
        at = slice(TILE * j, TILE * (j + 1))
        for copy in tokens[PER * j : PER * (j + 1)]:
            copy.wait()
        part = dot(w_ref[...], x_buf[PER * j : PER * (j + 1)].reshape(TILE, COLS), 1, 1)
        x = x_buf[PER * j : PER * (j + 1)].reshape(TILE, COLS).astype(F32)
        pivot = x[:, 0:1]
        c = x - pivot
        sq = jnp.sum(c * c, axis=1, keepdims=True)
        lane = iota((TILE, 128), 1)
        stat = jnp.where(lane == 0, sq, jnp.where(lane == 1, pivot, 0.0)).T
        m_row = part[UNITS : UNITS + 1] * (1.0 / COLS)
        off = m_row - stat[1:2]
        m2_row = stat[0:1] - COLS * off * off
        m_hi = rounded(m_row)
        m_mid = rounded(m_row - m_hi)
        m_lo = m_row - m_hi - m_mid
        m2_hi = rounded(m2_row)
        m2_lo = m2_row - m2_hi
        r = iota((8, TILE), 0)
        t1 = jnp.where(r == 4, m_hi, jnp.where(r == 5, m_mid, jnp.where(r == 6, m_lo, jnp.where(r == 7, vec_ref[0:1, at], 0.0))))
        t2 = jnp.where(r == 4, m2_hi, jnp.where(r == 5, m2_lo, jnp.where(r == 6, vec_ref[1:2, at], 0.0)))
        z = jnp.zeros((SLOT - 8, TILE), F32)
        extra = jnp.concatenate([z, t1, z, t2], axis=0)
        for k in range(4):
            rows = slice(PART * k, PART * (k + 1))
            out_buf[k, :, at] = (part[rows] - col[rows] * m_row + extra).astype(BF16)
        stores.append(pltpu.make_async_copy(out_buf.at[:, :, at], out_ref.at[:, :, at], sems.at[8 + j]))
        stores[-1].start()
    for copy in stores:
        copy.wait()


def project(tokens, gate_t, up_t, gain, bias):
    hbm = pl.BlockSpec(memory_space=pl.ANY)
    return pl.pallas_call(
        project_kernel,
        in_specs=[hbm] * 5,
        out_specs=hbm,
        out_shape=pltpu.HBM((4, PART, ROWS), BF16),
        scratch_shapes=[
            pltpu.VMEM((4, 4, 4, 16, COLS), BF16),
            pltpu.VMEM((FFL, COLS), F32),
            pltpu.VMEM((FFL, COLS), F32),
            pltpu.VMEM((2, 1, COLS), F32),
            pltpu.VMEM((4, PART, ROWS), BF16),
            pltpu.VMEM((4 * PART, COLS), BF16),
            pltpu.VMEM((8, ROWS), F32),
            pltpu.SemaphoreType.DMA((12,)),
        ],
        name="project",
    )(*[pltpu.with_memory_space_constraint(a, pltpu.HBM) for a in (tokens.reshape(4, 2, 4, 2, 16, COLS), gate_t, up_t, gain, bias)])


def hidden_kernel(r_ref, gs_ref, us_ref, out_ref, stat_ref):
    me = lax.axis_index("cb")
    means = []
    m2s = []
    for c in range(4):
        a = r_ref[c, 32:48, :].astype(F32)
        b = r_ref[c, 80:96, :].astype(F32)
        means.append(a[12:13] + a[13:14] + a[14:15])
        m2s.append(b[12:13] + b[13:14])
    mean = (means[0] + means[1] + means[2] + means[3]) * 0.25
    deltas = [v - mean for v in means]
    m2 = sum(m2s) + COLS * sum(d * d for d in deltas)
    rstd = lax.rsqrt(m2 * (1.0 / D) + 1e-05)
    q = iota((8, ROWS), 0)
    stat_ref[...] = jnp.where(q == 0, mean, jnp.where(q == 1, rstd, 0.0))

    wide = 8 * PART
    pick_row = iota((2 * PART, wide), 0)
    pick_lane = iota((2 * PART, wide), 1)
    base = jnp.where(pick_row < PART, me * PART, (4 + me) * PART - PART)
    pick = one_hot(pick_lane == pick_row + base)
    tiles = [r_ref[c, 32:48, 0:wide] for c in range(4)] + [r_ref[c, 80:96, 0:wide] for c in range(4)]
    vecs = dot(pick, jnp.concatenate(tiles, axis=0), 1, 1)
    col_sums = [vecs[0:PART, 16 * c + 15 : 16 * c + 16] + vecs[0:PART, 78 + 16 * c : 79 + 16 * c] for c in range(4)]
    biases = sum(vecs[PART:, 16 * c + 15 : 16 * c + 16] + vecs[PART:, 78 + 16 * c : 79 + 16 * c] for c in range(4))

    gs = gs_ref[...]
    us = us_ref[...]
    g1 = rounded(gs)
    g2 = rounded(gs - g1)
    u1 = rounded(us)
    u2 = rounded(us - u1)
    sr = iota((16, FFL), 0)
    pieces = jnp.where(sr == 0, g1, jnp.where(sr == 1, g2, jnp.where(sr == 2, gs - g1 - g2, 0.0)))
    pieces = pieces + jnp.where(sr == 3, u1, jnp.where(sr == 4, u2, jnp.where(sr == 5, us - u1 - u2, 0.0)))
    row = iota((PART, FFL), 0)
    unit = jnp.where(row < SLOT, row, row - SLOT)
    own = one_hot((iota((PART, FFL), 1) == unit + me * UNITS) & (unit < UNITS))
    sc = dot(own, pieces.astype(BF16), 1, 1)
    scale = jnp.where(iota((PART, 1), 0) < SLOT, sc[:, 0:1] + sc[:, 1:2] + sc[:, 2:3], sc[:, 3:4] + sc[:, 4:5] + sc[:, 5:6])

    keep = iota((SLOT, CHUNK), 0) < UNITS
    for j in range(4):
        at = slice(CHUNK * j, CHUNK * (j + 1))
        acc = jnp.zeros((PART, CHUNK), F32)
        for c in range(4):
            acc = acc + (r_ref[c, :, at].astype(F32) + col_sums[c] * deltas[c][:, at])
        y = (acc * rstd[:, at] + biases) * scale
        gate = y[0:SLOT]
        up = y[SLOT:PART]
        h = jnp.where(keep, gate / (1.0 + jnp.exp(-gate)) * up, 0.0).astype(BF16)
        for k in range(4):
            out_ref[j, k] = h


def hidden_of(received, gate_scale, up_scale):
    vm = pl.BlockSpec(memory_space=pltpu.VMEM)
    return pl.pallas_call(
        hidden_kernel,
        in_specs=[vm, vm, vm],
        out_specs=[vm, vm],
        out_shape=[pltpu.VMEM((4, 4, SLOT, CHUNK), BF16), pltpu.VMEM((8, ROWS), F32)],
        name="hidden",
    )(*[near(a) for a in (received, gate_scale, up_scale)])


def down_kernel(h_ref, own_ref, beside_ref, other_ref, across_ref, out_ref):
    me = lax.axis_index("zl") * 2 + lax.axis_index("yl")
    core = lax.axis_index("dp")

    unit = iota((FFL, 4 * SLOT), 0)
    slot = jnp.where(unit < 2 * UNITS, jnp.where(unit < UNITS, 0, 1), jnp.where(unit < 3 * UNITS, 2, 3))
    place = one_hot(iota((FFL, 4 * SLOT), 1) == unit + (SLOT - UNITS) * slot)

    def squeezed(member):
        return dot(h_ref[member], place, 0, 1).astype(BF16)

    acc = dot(squeezed(me), own_ref[...], 1, 0)
    acc = acc + dot(squeezed(me ^ (1 + core)), beside_ref[...], 1, 0)
    acc = acc + dot(squeezed(me ^ (2 - core)), other_ref[...], 1, 0)
    acc = acc + dot(squeezed(me ^ 3), across_ref[...], 1, 0)
    out_ref[...] = acc.astype(BF16)


def down(hidden, weights):
    vm = pl.BlockSpec(memory_space=pltpu.VMEM)
    return pl.pallas_call(
        down_kernel,
        in_specs=[vm] * 5,
        out_specs=vm,
        out_shape=pltpu.VMEM((CHUNK, COLS), BF16),
        name="down",
    )(near(hidden), *[near(w) for w in weights])


def mix_kernel(r_ref, x_ref, stat_ref, gain_ref, bias_ref, scale_ref, mixed_ref, part_ref):
    member = lax.axis_index("zl") * 2 + lax.axis_index("yl")
    at = member * CHUNK + (lax.axis_index("Z") * 4 + lax.axis_index("Y")) * 16
    branch = jnp.zeros((16, COLS), F32)
    for k in range(16):
        branch = branch + r_ref[k].astype(F32)
    mine = iota((16, ROWS), 1) == iota((16, ROWS), 0) + at
    mean = jnp.sum(jnp.where(mine, stat_ref[0:1], 0.0), axis=1, keepdims=True)
    rstd = jnp.sum(jnp.where(mine, stat_ref[1:2], 0.0), axis=1, keepdims=True)
    normed = rounded((x_ref[...].astype(F32) - mean) * rstd * gain_ref[...] + bias_ref[...])
    mixed = 0.5 * normed + branch * scale_ref[...]
    mixed_ref[...] = mixed
    m = jnp.sum(mixed, axis=1, keepdims=True) * (1.0 / COLS)
    c = mixed - m
    m2 = jnp.sum(c * c, axis=1, keepdims=True)
    lane = iota((16, 128), 1)
    part = jnp.where(lane == 0, m, jnp.where(lane == 1, m2, 0.0))
    for k in range(4):
        part_ref[k] = part


def mix(received, own, stats, gain, bias, scale):
    vm = pl.BlockSpec(memory_space=pltpu.VMEM)
    return pl.pallas_call(
        mix_kernel,
        in_specs=[vm] * 6,
        out_specs=[vm, vm],
        out_shape=[pltpu.VMEM((16, COLS), F32), pltpu.VMEM((4, 16, 128), F32)],
        name="mix",
    )(*[near(a) for a in (received, own, stats, gain, bias, scale)])


def finish_kernel(mixed_ref, part_ref, gain_ref, bias_ref, out_ref):
    parts = [part_ref[k] for k in range(4)]
    means = [p[:, 0:1] for p in parts]
    mean = (means[0] + means[1] + means[2] + means[3]) * 0.25
    m2 = sum(p[:, 1:2] for p in parts) + COLS * sum((v - mean) * (v - mean) for v in means)
    rstd = lax.rsqrt(m2 * (1.0 / D) + 1e-05)
    out_ref[...] = ((mixed_ref[...] - mean) * rstd * gain_ref[...] + bias_ref[...]).astype(BF16)


def finish(mixed, parts, gain, bias):
    vm = pl.BlockSpec(memory_space=pltpu.VMEM)
    return pl.pallas_call(
        finish_kernel,
        in_specs=[vm] * 4,
        out_specs=vm,
        out_shape=jax.ShapeDtypeStruct((16, COLS), BF16),
        name="finish",
    )(*[near(a) for a in (mixed, parts, gain, bias)])


def swapped(n, k):
    return [(i, i ^ k) for i in range(n)]


def local(
    tokens,
    norm_gain,
    norm_bias,
    gate_weight,
    up_weight,
    gate_scale,
    up_scale,
    down_weight,
    down_scale,
    out_gain,
    out_bias,
):
    gain = norm_gain.reshape(1, COLS)
    bias = norm_bias.reshape(1, COLS)

    w0 = down_weight.astype(BF16)
    beside = lax.ppermute(w0, ("zl", "yl", "dp"), [(i, i ^ (4 if i & 1 else 2)) for i in range(8)])
    across = lax.ppermute(w0, ("zl", "yl"), swapped(4, 3))
    other = lax.ppermute(beside, "dp", swapped(2, 1))

    shares = project(tokens, gate_weight.T, up_weight.T, gain, bias)
    received = lax.all_to_all(shares, "cb", 0, 0, tiled=True)
    sent, stats = hidden_of(received, gate_scale.reshape(1, FFL), up_scale.reshape(1, FFL))
    own = lax.dynamic_slice_in_dim(tokens, lax.axis_index(RA) * 16, 16, 0)
    sent, own = lax.optimization_barrier((sent, own))
    hidden = lax.all_to_all(sent.reshape(16, SLOT, CHUNK), ("zl", "yl", "cb"), 0, 0, tiled=True)
    partial = down(hidden.reshape(4, 4 * SLOT, CHUNK), (w0, beside, other, across))
    pieces = lax.all_to_all(partial.reshape(16, 16, COLS), ("Z", "Y"), 0, 0, tiled=True)
    mixed, part = mix(pieces, own, stats, gain, bias, down_scale.reshape(1, COLS))
    parts = lax.all_to_all(part, "cb", 0, 0, tiled=True)
    return finish(mixed, parts, out_gain.reshape(1, COLS), out_bias.reshape(1, COLS))


def solution(mesh):
    split = Mesh(mesh.devices.reshape(4, 2, 4, 2, 4, 2), RA + ("cb", "dp"))
    return jax.shard_map(
        local,
        mesh=split,
        in_specs=(
            P("dp", "cb"),
            P("cb"),
            P("cb"),
            P("cb", RA),
            P("cb", RA),
            P(RA),
            P(RA),
            P(RA, "cb"),
            P("cb"),
            P("cb"),
            P("cb"),
        ),
        out_specs=P(("dp",) + RA, "cb"),
        check_vma=False,
    )
```

```python
import jax
import jax.numpy as jnp
from jax import lax
from jax.experimental import pallas as pl
from jax.experimental.pallas import tpu as pltpu
from jax.sharding import Mesh, PartitionSpec as P


D = 4096
F32 = jnp.float32
BF16 = jnp.bfloat16
RA = ("Z", "zl", "Y", "yl")
UNITS = 44
SLOT = 48
PART = 2 * SLOT
ROWS = 1024
COLS = 1024
FFL = 176
CHUNK = 256
PER = 2
TILE = PER * CHUNK


def iota(shape, dim):
    return lax.broadcasted_iota(jnp.int32, shape, dim)


def near(a):
    return pltpu.with_memory_space_constraint(a, pltpu.VMEM)


def dot(a, b, ca, cb):
    return lax.dot_general(a, b, (((ca,), (cb,)), ((), ())), preferred_element_type=F32)


def rounded(v):
    return v.astype(BF16).astype(F32)


def one_hot(cond):
    return jnp.where(cond, 1.0, 0.0).astype(BF16)


def project_kernel(x_ref, gw_ref, uw_ref, gain_ref, bias_ref, out_ref, x_buf, gw_buf, uw_buf, gb_buf, out_buf, w_ref, vec_ref, sems):
    loads = [
        pltpu.make_async_copy(gw_ref, gw_buf, sems.at[0]),
        pltpu.make_async_copy(uw_ref, uw_buf, sems.at[1]),
        pltpu.make_async_copy(gain_ref, gb_buf.at[0], sems.at[2]),
        pltpu.make_async_copy(bias_ref, gb_buf.at[1], sems.at[3]),
    ]
    tokens = [
        pltpu.make_async_copy(x_ref.at[z, (j // 2) ^ flipped(z), :, j % 2], x_buf.at[j, z], sems.at[4 + 4 * j + z])
        for j in range(4)
        for z in range(4)
    ]
    for copy in loads + tokens[: 4 * PER]:
        copy.start()
    for copy in loads:
        copy.wait()
    for copy in tokens[4 * PER :]:
        copy.start()

    gain = gb_buf[0]
    row = iota((SLOT, COLS), 0)
    for k in range(4):
        first = UNITS * k - 4 * (k % 2)
        for half, ref in enumerate((gw_buf, uw_buf)):
            w = ref[first : min(first + SLOT + 8 * (k % 2), FFL)] * gain
            if k % 2:
                w = pltpu.roll(w, w.shape[0] - 4, 0)
            fill = jnp.where(row == UNITS, 1.0, 0.0) if half == 0 else 0.0
            at = PART * k + SLOT * half
            w_ref[at : at + SLOT, :] = jnp.where(row < UNITS, w[0:SLOT], fill).astype(BF16)
    r = iota((128, COLS), 0)
    ratio = gb_buf[1] / gain
    rh = rounded(ratio)
    lead = jnp.where(r == 0, 1.0, jnp.where(r == 1, rh, jnp.where(r == 2, ratio - rh, 0.0))).astype(BF16)
    cols = dot(w_ref[...], lead, 1, 1)
    col = cols[:, 0:1]
    sums = cols.T
    both = jnp.concatenate([sums[0:1], sums[1:2] + sums[2:3], jnp.zeros((1, ROWS - 8 * PART), F32)], axis=1)
    hi = rounded(both)
    q = iota((8, ROWS), 0)
    vec_ref[...] = jnp.where(q == 0, hi, jnp.where(q == 1, both - hi, 0.0))

    stores = []
    for j in range(4 // PER):
        at = slice(TILE * j, TILE * (j + 1))
        for copy in tokens[4 * PER * j : 4 * PER * (j + 1)]:
            copy.wait()
        part = dot(w_ref[...], x_buf[PER * j : PER * (j + 1)].reshape(TILE, COLS), 1, 1)
        x = x_buf[PER * j : PER * (j + 1)].reshape(TILE, COLS).astype(F32)
        pivot = x[:, 0:1]
        c = x - pivot
        sq = jnp.sum(c * c, axis=1, keepdims=True)
        lane = iota((TILE, 128), 1)
        stat = jnp.where(lane == 0, sq, jnp.where(lane == 1, pivot, 0.0)).T
        m_row = part[UNITS : UNITS + 1] * (1.0 / COLS)
        off = m_row - stat[1:2]
        m2_row = stat[0:1] - COLS * off * off
        m_hi = rounded(m_row)
        m_mid = rounded(m_row - m_hi)
        m_lo = m_row - m_hi - m_mid
        m2_hi = rounded(m2_row)
        m2_lo = m2_row - m2_hi
        r = iota((8, TILE), 0)
        t1 = jnp.where(r == 4, m_hi, jnp.where(r == 5, m_mid, jnp.where(r == 6, m_lo, jnp.where(r == 7, vec_ref[0:1, at], 0.0))))
        t2 = jnp.where(r == 4, m2_hi, jnp.where(r == 5, m2_lo, jnp.where(r == 6, vec_ref[1:2, at], 0.0)))
        z = jnp.zeros((SLOT - 8, TILE), F32)
        extra = jnp.concatenate([z, t1, z, t2], axis=0)
        for k in range(4):
            rows = slice(PART * k, PART * (k + 1))
            out_buf[k, :, at] = (part[rows] - col[rows] * m_row + extra).astype(BF16)
        stores.append(pltpu.make_async_copy(out_buf.at[:, :, at], out_ref.at[:, :, at], sems.at[20 + j]))
        stores[-1].start()
    for copy in stores:
        copy.wait()


def project(tokens, gate_t, up_t, gain, bias):
    hbm = pl.BlockSpec(memory_space=pl.ANY)
    return pl.pallas_call(
        project_kernel,
        in_specs=[hbm] * 5,
        out_specs=hbm,
        out_shape=pltpu.HBM((4, PART, ROWS), BF16),
        scratch_shapes=[
            pltpu.VMEM((4, 4, 4, 16, COLS), BF16),
            pltpu.VMEM((FFL, COLS), F32),
            pltpu.VMEM((FFL, COLS), F32),
            pltpu.VMEM((2, 1, COLS), F32),
            pltpu.VMEM((4, PART, ROWS), BF16),
            pltpu.VMEM((4 * PART, COLS), BF16),
            pltpu.VMEM((8, ROWS), F32),
            pltpu.SemaphoreType.DMA((24,)),
        ],
        name="project",
    )(*[pltpu.with_memory_space_constraint(a, pltpu.HBM) for a in (tokens.reshape(4, 2, 4, 2, 16, COLS), gate_t, up_t, gain, bias)])


def hidden_kernel(r_ref, gs_ref, us_ref, out_ref, stat_ref):
    me = lax.axis_index("cb")
    means = []
    m2s = []
    for c in range(4):
        a = r_ref[c, 32:48, :].astype(F32)
        b = r_ref[c, 80:96, :].astype(F32)
        means.append(a[12:13] + a[13:14] + a[14:15])
        m2s.append(b[12:13] + b[13:14])
    mean = (means[0] + means[1] + means[2] + means[3]) * 0.25
    deltas = [v - mean for v in means]
    m2 = sum(m2s) + COLS * sum(d * d for d in deltas)
    rstd = lax.rsqrt(m2 * (1.0 / D) + 1e-05)
    q = iota((8, ROWS), 0)
    stat_ref[...] = jnp.where(q == 0, mean, jnp.where(q == 1, rstd, 0.0))

    wide = 8 * PART
    pick_row = iota((2 * PART, wide), 0)
    pick_lane = iota((2 * PART, wide), 1)
    base = jnp.where(pick_row < PART, me * PART, (4 + me) * PART - PART)
    pick = one_hot(pick_lane == pick_row + base)
    tiles = [r_ref[c, 32:48, 0:wide] for c in range(4)] + [r_ref[c, 80:96, 0:wide] for c in range(4)]
    vecs = dot(pick, jnp.concatenate(tiles, axis=0), 1, 1)
    col_sums = [vecs[0:PART, 16 * c + 15 : 16 * c + 16] + vecs[0:PART, 78 + 16 * c : 79 + 16 * c] for c in range(4)]
    biases = sum(vecs[PART:, 16 * c + 15 : 16 * c + 16] + vecs[PART:, 78 + 16 * c : 79 + 16 * c] for c in range(4))

    gs = gs_ref[...]
    us = us_ref[...]
    g1 = rounded(gs)
    g2 = rounded(gs - g1)
    u1 = rounded(us)
    u2 = rounded(us - u1)
    sr = iota((16, FFL), 0)
    pieces = jnp.where(sr == 0, g1, jnp.where(sr == 1, g2, jnp.where(sr == 2, gs - g1 - g2, 0.0)))
    pieces = pieces + jnp.where(sr == 3, u1, jnp.where(sr == 4, u2, jnp.where(sr == 5, us - u1 - u2, 0.0)))
    row = iota((PART, FFL), 0)
    unit = jnp.where(row < SLOT, row, row - SLOT)
    own = one_hot((iota((PART, FFL), 1) == unit + me * UNITS) & (unit < UNITS))
    sc = dot(own, pieces.astype(BF16), 1, 1)
    scale = jnp.where(iota((PART, 1), 0) < SLOT, sc[:, 0:1] + sc[:, 1:2] + sc[:, 2:3], sc[:, 3:4] + sc[:, 4:5] + sc[:, 5:6])

    keep = iota((SLOT, CHUNK), 0) < UNITS
    turn = 2 * flipped(lax.axis_index("Z"))
    for j in range(4):
        at = slice(CHUNK * j, CHUNK * (j + 1))
        acc = jnp.zeros((PART, CHUNK), F32)
        for c in range(4):
            acc = acc + (r_ref[c, :, at].astype(F32) + col_sums[c] * deltas[c][:, at])
        y = (acc * rstd[:, at] + biases) * scale
        gate = y[0:SLOT]
        up = y[SLOT:PART]
        h = jnp.where(keep, gate / (1.0 + jnp.exp(-gate)) * up, 0.0).astype(BF16)
        for k in range(4):
            out_ref[j ^ turn, k] = h


def hidden_of(received, gate_scale, up_scale):
    vm = pl.BlockSpec(memory_space=pltpu.VMEM)
    return pl.pallas_call(
        hidden_kernel,
        in_specs=[vm, vm, vm],
        out_specs=[vm, vm],
        out_shape=[pltpu.VMEM((4, 4, SLOT, CHUNK), BF16), pltpu.VMEM((8, ROWS), F32)],
        name="hidden",
    )(*[near(a) for a in (received, gate_scale, up_scale)])


def down_kernel(h_ref, own_ref, fetched_ref, other_ref, out_ref):
    me = lax.axis_index("zl") * 2 + lax.axis_index("yl")
    core = lax.axis_index("dp")

    unit = iota((FFL, 4 * SLOT), 0)
    slot = jnp.where(unit < 2 * UNITS, jnp.where(unit < UNITS, 0, 1), jnp.where(unit < 3 * UNITS, 2, 3))
    place = one_hot(iota((FFL, 4 * SLOT), 1) == unit + (SLOT - UNITS) * slot)

    def squeezed(member):
        return dot(h_ref[member], place, 0, 1).astype(BF16)

    acc = dot(squeezed(me), own_ref[...], 1, 0)
    acc = acc + dot(squeezed(me ^ (1 + core)), fetched_ref[:, 0:COLS], 1, 0)
    acc = acc + dot(squeezed(me ^ (2 - core)), other_ref[:, 0:COLS], 1, 0)
    h = squeezed(me ^ 3)
    mine = dot(h, fetched_ref[:, COLS:], 1, 0)
    theirs = dot(h, other_ref[:, COLS:], 1, 0)
    acc = acc + jnp.concatenate([jnp.where(core == 0, mine, theirs), jnp.where(core == 0, theirs, mine)], axis=1)
    out_ref[...] = acc.astype(BF16)


def down(hidden, weights):
    vm = pl.BlockSpec(memory_space=pltpu.VMEM)
    return pl.pallas_call(
        down_kernel,
        in_specs=[vm] * 4,
        out_specs=vm,
        out_shape=pltpu.VMEM((CHUNK, COLS), BF16),
        name="down",
    )(near(hidden), *[near(w) for w in weights])


def mix_kernel(r_ref, x_ref, stat_ref, gain_ref, bias_ref, scale_ref, mixed_ref, part_ref):
    member = (lax.axis_index("zl") ^ flipped(lax.axis_index("Z"))) * 2 + lax.axis_index("yl")
    at = member * CHUNK + (lax.axis_index("Z") * 4 + lax.axis_index("Y")) * 16
    branch = jnp.zeros((16, COLS), F32)
    for k in range(16):
        branch = branch + r_ref[k].astype(F32)
    mine = iota((16, ROWS), 1) == iota((16, ROWS), 0) + at
    mean = jnp.sum(jnp.where(mine, stat_ref[0:1], 0.0), axis=1, keepdims=True)
    rstd = jnp.sum(jnp.where(mine, stat_ref[1:2], 0.0), axis=1, keepdims=True)
    normed = rounded((x_ref[...].astype(F32) - mean) * rstd * gain_ref[...] + bias_ref[...])
    mixed = 0.5 * normed + branch * scale_ref[...]
    mixed_ref[...] = mixed
    m = jnp.sum(mixed, axis=1, keepdims=True) * (1.0 / COLS)
    c = mixed - m
    m2 = jnp.sum(c * c, axis=1, keepdims=True)
    lane = iota((16, 128), 1)
    part = jnp.where(lane == 0, m, jnp.where(lane == 1, m2, 0.0))
    for k in range(4):
        part_ref[k] = part


def mix(received, own, stats, gain, bias, scale):
    vm = pl.BlockSpec(memory_space=pltpu.VMEM)
    return pl.pallas_call(
        mix_kernel,
        in_specs=[vm] * 6,
        out_specs=[vm, vm],
        out_shape=[pltpu.VMEM((16, COLS), F32), pltpu.VMEM((4, 16, 128), F32)],
        name="mix",
    )(*[near(a) for a in (received, own, stats, gain, bias, scale)])


def finish_kernel(mixed_ref, part_ref, gain_ref, bias_ref, out_ref):
    parts = [part_ref[k] for k in range(4)]
    means = [p[:, 0:1] for p in parts]
    mean = (means[0] + means[1] + means[2] + means[3]) * 0.25
    m2 = sum(p[:, 1:2] for p in parts) + COLS * sum((v - mean) * (v - mean) for v in means)
    rstd = lax.rsqrt(m2 * (1.0 / D) + 1e-05)
    out_ref[...] = ((mixed_ref[...] - mean) * rstd * gain_ref[...] + bias_ref[...]).astype(BF16)


def finish(mixed, parts, gain, bias):
    vm = pl.BlockSpec(memory_space=pltpu.VMEM)
    return pl.pallas_call(
        finish_kernel,
        in_specs=[vm] * 4,
        out_specs=vm,
        out_shape=jax.ShapeDtypeStruct((16, COLS), BF16),
        name="finish",
    )(*[near(a) for a in (mixed, parts, gain, bias)])


def flipped(z):
    return (z ^ (z >> 1)) & 1


def spread_groups():
    return [
        [(2 * z + (jz ^ flipped(z))) * 8 + 2 * y + jy for z in range(4) for y in range(4)]
        for jz in range(2)
        for jy in range(2)
    ]


def swapped(n, k):
    return [(i, i ^ k) for i in range(n)]


def local(
    tokens,
    norm_gain,
    norm_bias,
    gate_weight,
    up_weight,
    gate_scale,
    up_scale,
    down_weight,
    down_scale,
    out_gain,
    out_bias,
):
    gain = norm_gain.reshape(1, COLS)
    bias = norm_bias.reshape(1, COLS)

    w0 = down_weight.astype(BF16)
    beside = lax.ppermute(w0, ("zl", "yl", "dp"), [(i, i ^ (4 if i & 1 else 2)) for i in range(8)])
    half = lax.dynamic_slice_in_dim(w0, lax.axis_index("dp") * (COLS // 2), COLS // 2, 1)
    across = lax.ppermute(half, ("zl", "yl"), swapped(4, 3))

    shares = project(tokens, gate_weight.T, up_weight.T, gain, bias)
    received = lax.all_to_all(shares, "cb", 0, 0, tiled=True)
    sent, stats = hidden_of(received, gate_scale.reshape(1, FFL), up_scale.reshape(1, FFL))
    own = lax.dynamic_slice_in_dim(tokens, lax.axis_index(RA) * 16, 16, 0)
    sent, own = lax.optimization_barrier((sent, own))
    hidden = lax.all_to_all(sent.reshape(16, SLOT, CHUNK), ("zl", "yl", "cb"), 0, 0, tiled=True)
    fetched = jnp.concatenate([beside, across], axis=1)
    other = lax.ppermute(fetched, "dp", swapped(2, 1))
    partial = down(hidden.reshape(4, 4 * SLOT, CHUNK), (w0, fetched, other))
    pieces = lax.all_to_all(
        partial.reshape(16, 16, COLS), RA, 0, 0, axis_index_groups=spread_groups(), tiled=True
    )
    mixed, part = mix(pieces, own, stats, gain, bias, down_scale.reshape(1, COLS))
    parts = lax.all_to_all(part, "cb", 0, 0, tiled=True)
    return finish(mixed, parts, out_gain.reshape(1, COLS), out_bias.reshape(1, COLS))


def solution(mesh):
    split = Mesh(mesh.devices.reshape(4, 2, 4, 2, 4, 2), RA + ("cb", "dp"))
    return jax.shard_map(
        local,
        mesh=split,
        in_specs=(
            P("dp", "cb"),
            P("cb"),
            P("cb"),
            P("cb", RA),
            P("cb", RA),
            P(RA),
            P(RA),
            P(RA, "cb"),
            P("cb"),
            P("cb"),
            P("cb"),
        ),
        out_specs=P(("dp",) + RA, "cb"),
        check_vma=False,
    )
```

```python
import jax
import jax.numpy as jnp
from jax import lax
from jax.experimental import pallas as pl
from jax.experimental.pallas import tpu as pltpu
from jax.sharding import Mesh, PartitionSpec as P


D = 4096
F32 = jnp.float32
BF16 = jnp.bfloat16
RA = ("Z", "zl", "Y", "yl")
UNITS = 44
SLOT = 48
PART = 2 * SLOT
ROWS = 1024
COLS = 1024
FFL = 176
CHUNK = 256
PER = 2
TILE = PER * CHUNK


def iota(shape, dim):
    return lax.broadcasted_iota(jnp.int32, shape, dim)


def near(a):
    return pltpu.with_memory_space_constraint(a, pltpu.VMEM)


def dot(a, b, ca, cb):
    return lax.dot_general(a, b, (((ca,), (cb,)), ((), ())), preferred_element_type=F32)


def rounded(v):
    return v.astype(BF16).astype(F32)


def one_hot(cond):
    return jnp.where(cond, 1.0, 0.0).astype(BF16)


def project_kernel(x_ref, gw_ref, uw_ref, gain_ref, bias_ref, out_ref, x_buf, gw_buf, uw_buf, gb_buf, out_buf, w_ref, vec_ref, sems):
    loads = [
        pltpu.make_async_copy(gw_ref, gw_buf, sems.at[0]),
        pltpu.make_async_copy(uw_ref, uw_buf, sems.at[1]),
        pltpu.make_async_copy(gain_ref, gb_buf.at[0], sems.at[2]),
        pltpu.make_async_copy(bias_ref, gb_buf.at[1], sems.at[3]),
    ]
    runs = ((0, 1), (1, 3), (3, 4))
    tokens = [
        pltpu.make_async_copy(x_ref.at[a:b, (j // 2) ^ flipped(a), :, j % 2], x_buf.at[j, a:b], sems.at[4 + 3 * j + i])
        for j in range(4)
        for i, (a, b) in enumerate(runs)
    ]
    for copy in loads + tokens[: 3 * PER]:
        copy.start()
    for copy in loads:
        copy.wait()
    for copy in tokens[3 * PER :]:
        copy.start()

    gain = gb_buf[0]
    row = iota((SLOT, COLS), 0)
    for k in range(4):
        first = UNITS * k - 4 * (k % 2)
        for half, ref in enumerate((gw_buf, uw_buf)):
            w = ref[first : min(first + SLOT + 8 * (k % 2), FFL)] * gain
            if k % 2:
                w = pltpu.roll(w, w.shape[0] - 4, 0)
            fill = jnp.where(row == UNITS, 1.0, 0.0) if half == 0 else 0.0
            at = PART * k + SLOT * half
            w_ref[at : at + SLOT, :] = jnp.where(row < UNITS, w[0:SLOT], fill).astype(BF16)
    r = iota((128, COLS), 0)
    ratio = gb_buf[1] / gain
    rh = rounded(ratio)
    lead = jnp.where(r == 0, 1.0, jnp.where(r == 1, rh, jnp.where(r == 2, ratio - rh, 0.0))).astype(BF16)
    cols = dot(w_ref[...], lead, 1, 1)
    col = cols[:, 0:1]
    sums = cols.T
    both = jnp.concatenate([sums[0:1], sums[1:2] + sums[2:3], jnp.zeros((1, ROWS - 8 * PART), F32)], axis=1)
    hi = rounded(both)
    q = iota((8, ROWS), 0)
    vec_ref[...] = jnp.where(q == 0, hi, jnp.where(q == 1, both - hi, 0.0))

    stores = []
    for j in range(4 // PER):
        at = slice(TILE * j, TILE * (j + 1))
        for copy in tokens[3 * PER * j : 3 * PER * (j + 1)]:
            copy.wait()
        part = dot(w_ref[...], x_buf[PER * j : PER * (j + 1)].reshape(TILE, COLS), 1, 1)
        x = x_buf[PER * j : PER * (j + 1)].reshape(TILE, COLS).astype(F32)
        pivot = x[:, 0:1]
        c = x - pivot
        sq = jnp.sum(c * c, axis=1, keepdims=True)
        lane = iota((TILE, 128), 1)
        stat = jnp.where(lane == 0, sq, jnp.where(lane == 1, pivot, 0.0)).T
        m_row = part[UNITS : UNITS + 1] * (1.0 / COLS)
        off = m_row - stat[1:2]
        m2_row = stat[0:1] - COLS * off * off
        m_hi = rounded(m_row)
        m_mid = rounded(m_row - m_hi)
        m_lo = m_row - m_hi - m_mid
        m2_hi = rounded(m2_row)
        m2_lo = m2_row - m2_hi
        r = iota((8, TILE), 0)
        t1 = jnp.where(r == 4, m_hi, jnp.where(r == 5, m_mid, jnp.where(r == 6, m_lo, jnp.where(r == 7, vec_ref[0:1, at], 0.0))))
        t2 = jnp.where(r == 4, m2_hi, jnp.where(r == 5, m2_lo, jnp.where(r == 6, vec_ref[1:2, at], 0.0)))
        z = jnp.zeros((SLOT - 8, TILE), F32)
        extra = jnp.concatenate([z, t1, z, t2], axis=0)
        for k in range(4):
            rows = slice(PART * k, PART * (k + 1))
            out_buf[k, :, at] = (part[rows] - col[rows] * m_row + extra).astype(BF16)
        stores.append(pltpu.make_async_copy(out_buf.at[:, :, at], out_ref.at[:, :, at], sems.at[20 + j]))
        stores[-1].start()
    for copy in stores:
        copy.wait()


def project(tokens, gate_t, up_t, gain, bias):
    hbm = pl.BlockSpec(memory_space=pl.ANY)
    return pl.pallas_call(
        project_kernel,
        in_specs=[hbm] * 5,
        out_specs=hbm,
        out_shape=pltpu.HBM((4, PART, ROWS), BF16),
        scratch_shapes=[
            pltpu.VMEM((4, 4, 4, 16, COLS), BF16),
            pltpu.VMEM((FFL, COLS), F32),
            pltpu.VMEM((FFL, COLS), F32),
            pltpu.VMEM((2, 1, COLS), F32),
            pltpu.VMEM((4, PART, ROWS), BF16),
            pltpu.VMEM((4 * PART, COLS), BF16),
            pltpu.VMEM((8, ROWS), F32),
            pltpu.SemaphoreType.DMA((24,)),
        ],
        name="project",
    )(*[pltpu.with_memory_space_constraint(a, pltpu.HBM) for a in (tokens.reshape(4, 2, 4, 2, 16, COLS), gate_t, up_t, gain, bias)])


def hidden_kernel(r_ref, gs_ref, us_ref, out_ref, stat_ref):
    me = lax.axis_index("cb")
    means = []
    m2s = []
    for c in range(4):
        a = r_ref[c, 32:48, :].astype(F32)
        b = r_ref[c, 80:96, :].astype(F32)
        means.append(a[12:13] + a[13:14] + a[14:15])
        m2s.append(b[12:13] + b[13:14])
    mean = (means[0] + means[1] + means[2] + means[3]) * 0.25
    deltas = [v - mean for v in means]
    m2 = sum(m2s) + COLS * sum(d * d for d in deltas)
    rstd = lax.rsqrt(m2 * (1.0 / D) + 1e-05)
    q = iota((8, ROWS), 0)
    stat_ref[...] = jnp.where(q == 0, mean, jnp.where(q == 1, rstd, 0.0))

    wide = 8 * PART
    pick_row = iota((2 * PART, wide), 0)
    pick_lane = iota((2 * PART, wide), 1)
    base = jnp.where(pick_row < PART, me * PART, (4 + me) * PART - PART)
    pick = one_hot(pick_lane == pick_row + base)
    tiles = [r_ref[c, 32:48, 0:wide] for c in range(4)] + [r_ref[c, 80:96, 0:wide] for c in range(4)]
    vecs = dot(pick, jnp.concatenate(tiles, axis=0), 1, 1)
    col_sums = [vecs[0:PART, 16 * c + 15 : 16 * c + 16] + vecs[0:PART, 78 + 16 * c : 79 + 16 * c] for c in range(4)]
    biases = sum(vecs[PART:, 16 * c + 15 : 16 * c + 16] + vecs[PART:, 78 + 16 * c : 79 + 16 * c] for c in range(4))

    gs = gs_ref[...]
    us = us_ref[...]
    g1 = rounded(gs)
    g2 = rounded(gs - g1)
    u1 = rounded(us)
    u2 = rounded(us - u1)
    sr = iota((16, FFL), 0)
    pieces = jnp.where(sr == 0, g1, jnp.where(sr == 1, g2, jnp.where(sr == 2, gs - g1 - g2, 0.0)))
    pieces = pieces + jnp.where(sr == 3, u1, jnp.where(sr == 4, u2, jnp.where(sr == 5, us - u1 - u2, 0.0)))
    row = iota((PART, FFL), 0)
    unit = jnp.where(row < SLOT, row, row - SLOT)
    own = one_hot((iota((PART, FFL), 1) == unit + me * UNITS) & (unit < UNITS))
    sc = dot(own, pieces.astype(BF16), 1, 1)
    scale = jnp.where(iota((PART, 1), 0) < SLOT, sc[:, 0:1] + sc[:, 1:2] + sc[:, 2:3], sc[:, 3:4] + sc[:, 4:5] + sc[:, 5:6])

    keep = iota((SLOT, CHUNK), 0) < UNITS
    turn = 2 * flipped(lax.axis_index("Z"))
    for j in range(4):
        at = slice(CHUNK * j, CHUNK * (j + 1))
        acc = jnp.zeros((PART, CHUNK), F32)
        for c in range(4):
            acc = acc + (r_ref[c, :, at].astype(F32) + col_sums[c] * deltas[c][:, at])
        y = (acc * rstd[:, at] + biases) * scale
        gate = y[0:SLOT]
        up = y[SLOT:PART]
        h = jnp.where(keep, gate / (1.0 + jnp.exp(-gate)) * up, 0.0).astype(BF16)
        for k in range(4):
            out_ref[k, j ^ turn] = h


def hidden_of(received, gate_scale, up_scale):
    vm = pl.BlockSpec(memory_space=pltpu.VMEM)
    return pl.pallas_call(
        hidden_kernel,
        in_specs=[vm, vm, vm],
        out_specs=[vm, vm],
        out_shape=[pltpu.VMEM((4, 4, SLOT, CHUNK), BF16), pltpu.VMEM((8, ROWS), F32)],
        name="hidden",
    )(*[near(a) for a in (received, gate_scale, up_scale)])


def down_kernel(h_ref, own_ref, fetched_ref, other_ref, out_ref):
    me = lax.axis_index("zl") * 2 + lax.axis_index("yl")
    core = lax.axis_index("dp")

    unit = iota((FFL, 4 * SLOT), 0)
    slot = jnp.where(unit < 2 * UNITS, jnp.where(unit < UNITS, 0, 1), jnp.where(unit < 3 * UNITS, 2, 3))
    place = one_hot(iota((FFL, 4 * SLOT), 1) == unit + (SLOT - UNITS) * slot)

    def squeezed(member):
        h = jnp.concatenate([h_ref[k, member] for k in range(4)], axis=0)
        return dot(h, place, 0, 1).astype(BF16)

    acc = dot(squeezed(me), own_ref[...], 1, 0)
    acc = acc + dot(squeezed(me ^ (1 + core)), fetched_ref[:, 0:COLS], 1, 0)
    acc = acc + dot(squeezed(me ^ (2 - core)), other_ref[:, 0:COLS], 1, 0)
    h = squeezed(me ^ 3)
    mine = dot(h, fetched_ref[:, COLS:], 1, 0)
    theirs = dot(h, other_ref[:, COLS:], 1, 0)
    acc = acc + jnp.concatenate([jnp.where(core == 0, mine, theirs), jnp.where(core == 0, theirs, mine)], axis=1)
    out_ref[...] = acc.astype(BF16)


def down(hidden, weights):
    vm = pl.BlockSpec(memory_space=pltpu.VMEM)
    return pl.pallas_call(
        down_kernel,
        in_specs=[vm] * 4,
        out_specs=vm,
        out_shape=pltpu.VMEM((CHUNK, COLS), BF16),
        name="down",
    )(near(hidden), *[near(w) for w in weights])


def mix_kernel(r_ref, x_ref, stat_ref, gain_ref, bias_ref, scale_ref, mixed_ref, part_ref):
    member = (lax.axis_index("zl") ^ flipped(lax.axis_index("Z"))) * 2 + lax.axis_index("yl")
    at = member * CHUNK + (lax.axis_index("Z") * 4 + lax.axis_index("Y")) * 16
    branch = jnp.zeros((16, COLS), F32)
    for k in range(16):
        branch = branch + r_ref[k].astype(F32)
    mine = iota((16, ROWS), 1) == iota((16, ROWS), 0) + at
    mean = jnp.sum(jnp.where(mine, stat_ref[0:1], 0.0), axis=1, keepdims=True)
    rstd = jnp.sum(jnp.where(mine, stat_ref[1:2], 0.0), axis=1, keepdims=True)
    normed = rounded((x_ref[...].astype(F32) - mean) * rstd * gain_ref[...] + bias_ref[...])
    mixed = 0.5 * normed + branch * scale_ref[...]
    mixed_ref[...] = mixed
    m = jnp.sum(mixed, axis=1, keepdims=True) * (1.0 / COLS)
    c = mixed - m
    m2 = jnp.sum(c * c, axis=1, keepdims=True)
    lane = iota((16, 128), 1)
    part = jnp.where(lane == 0, m, jnp.where(lane == 1, m2, 0.0))
    for k in range(4):
        part_ref[k] = part


def mix(received, own, stats, gain, bias, scale):
    vm = pl.BlockSpec(memory_space=pltpu.VMEM)
    return pl.pallas_call(
        mix_kernel,
        in_specs=[vm] * 6,
        out_specs=[vm, vm],
        out_shape=[pltpu.VMEM((16, COLS), F32), pltpu.VMEM((4, 16, 128), F32)],
        name="mix",
    )(*[near(a) for a in (received, own, stats, gain, bias, scale)])


def finish_kernel(mixed_ref, part_ref, gain_ref, bias_ref, out_ref):
    parts = [part_ref[k] for k in range(4)]
    means = [p[:, 0:1] for p in parts]
    mean = (means[0] + means[1] + means[2] + means[3]) * 0.25
    m2 = sum(p[:, 1:2] for p in parts) + COLS * sum((v - mean) * (v - mean) for v in means)
    rstd = lax.rsqrt(m2 * (1.0 / D) + 1e-05)
    out_ref[...] = ((mixed_ref[...] - mean) * rstd * gain_ref[...] + bias_ref[...]).astype(BF16)


def finish(mixed, parts, gain, bias):
    vm = pl.BlockSpec(memory_space=pltpu.VMEM)
    return pl.pallas_call(
        finish_kernel,
        in_specs=[vm] * 4,
        out_specs=vm,
        out_shape=jax.ShapeDtypeStruct((16, COLS), BF16),
        name="finish",
    )(*[near(a) for a in (mixed, parts, gain, bias)])


def flipped(z):
    return (z ^ (z >> 1)) & 1


def spread_groups():
    return [
        [(2 * z + (jz ^ flipped(z))) * 8 + 2 * y + jy for z in range(4) for y in range(4)]
        for jz in range(2)
        for jy in range(2)
    ]


def swapped(n, k):
    return [(i, i ^ k) for i in range(n)]


def local(
    tokens,
    norm_gain,
    norm_bias,
    gate_weight,
    up_weight,
    gate_scale,
    up_scale,
    down_weight,
    down_scale,
    out_gain,
    out_bias,
):
    gain = norm_gain.reshape(1, COLS)
    bias = norm_bias.reshape(1, COLS)

    w0 = down_weight.astype(BF16)
    beside = lax.ppermute(w0, ("zl", "yl", "dp"), [(i, i ^ (4 if i & 1 else 2)) for i in range(8)])
    half = lax.dynamic_slice_in_dim(w0, lax.axis_index("dp") * (COLS // 2), COLS // 2, 1)
    across = lax.ppermute(half, ("zl", "yl"), swapped(4, 3))

    shares = project(tokens, gate_weight.T, up_weight.T, gain, bias)
    received = lax.all_to_all(shares, "cb", 0, 0, tiled=True)
    sent, stats = hidden_of(received, gate_scale.reshape(1, FFL), up_scale.reshape(1, FFL))
    own = lax.dynamic_slice_in_dim(tokens, lax.axis_index(RA) * 16, 16, 0)
    sent, own = lax.optimization_barrier((sent, own))
    hidden = lax.all_to_all(sent.reshape(16, SLOT, CHUNK), ("cb", "zl", "yl"), 0, 0, tiled=True)
    fetched = jnp.concatenate([beside, across], axis=1)
    other = lax.ppermute(fetched, "dp", swapped(2, 1))
    partial = down(hidden.reshape(4, 4, SLOT, CHUNK), (w0, fetched, other))
    pieces = lax.all_to_all(
        partial.reshape(16, 16, COLS), RA, 0, 0, axis_index_groups=spread_groups(), tiled=True
    )
    mixed, part = mix(pieces, own, stats, gain, bias, down_scale.reshape(1, COLS))
    parts = lax.all_to_all(part, "cb", 0, 0, tiled=True)
    return finish(mixed, parts, out_gain.reshape(1, COLS), out_bias.reshape(1, COLS))


def solution(mesh):
    split = Mesh(mesh.devices.reshape(4, 2, 4, 2, 4, 2), RA + ("cb", "dp"))
    return jax.shard_map(
        local,
        mesh=split,
        in_specs=(
            P("dp", "cb"),
            P("cb"),
            P("cb"),
            P("cb", RA),
            P("cb", RA),
            P(RA),
            P(RA),
            P(RA, "cb"),
            P("cb"),
            P("cb"),
            P("cb"),
        ),
        out_specs=P(("dp",) + RA, "cb"),
        check_vma=False,
    )
```

```python
import jax
import jax.numpy as jnp
from jax import lax
from jax.experimental import pallas as pl
from jax.experimental.pallas import tpu as pltpu
from jax.sharding import Mesh, PartitionSpec as P


D = 4096
F32 = jnp.float32
BF16 = jnp.bfloat16
RA = ("Z", "zl", "Y", "yl")
UNITS = 44
SLOT = 48
PART = 2 * SLOT
ROWS = 1024
COLS = 1024
FFL = 176
CHUNK = 256
PER = 2
TILE = PER * CHUNK


def iota(shape, dim):
    return lax.broadcasted_iota(jnp.int32, shape, dim)


def near(a):
    return pltpu.with_memory_space_constraint(a, pltpu.VMEM)


def dot(a, b, ca, cb):
    return lax.dot_general(a, b, (((ca,), (cb,)), ((), ())), preferred_element_type=F32)


def rounded(v):
    return v.astype(BF16).astype(F32)


def one_hot(cond):
    return jnp.where(cond, 1.0, 0.0).astype(BF16)


def project_kernel(x_ref, gw_ref, uw_ref, gain_ref, bias_ref, out_ref, x_buf, gw_buf, uw_buf, gb_buf, out_buf, w_ref, vec_ref, sems):
    loads = [
        pltpu.make_async_copy(gw_ref, gw_buf, sems.at[0]),
        pltpu.make_async_copy(uw_ref, uw_buf, sems.at[1]),
        pltpu.make_async_copy(gain_ref, gb_buf.at[0], sems.at[2]),
        pltpu.make_async_copy(bias_ref, gb_buf.at[1], sems.at[3]),
    ]
    runs = ((0, 1), (1, 3), (3, 4))
    tokens = [
        pltpu.make_async_copy(
            x_ref.at[a:b, (j // 2) ^ flipped(a), c:d, (j % 2) ^ flipped(c)],
            x_buf.at[j, a:b, c:d],
            sems.at[4 + 9 * j + 3 * i + k],
        )
        for j in range(4)
        for i, (a, b) in enumerate(runs)
        for k, (c, d) in enumerate(runs)
    ]
    for copy in loads + tokens[: 9 * PER]:
        copy.start()
    for copy in loads:
        copy.wait()
    for copy in tokens[9 * PER :]:
        copy.start()

    gain = gb_buf[0]
    row = iota((SLOT, COLS), 0)
    for k in range(4):
        first = UNITS * k - 4 * (k % 2)
        for half, ref in enumerate((gw_buf, uw_buf)):
            w = ref[first : min(first + SLOT + 8 * (k % 2), FFL)] * gain
            if k % 2:
                w = pltpu.roll(w, w.shape[0] - 4, 0)
            fill = jnp.where(row == UNITS, 1.0, 0.0) if half == 0 else 0.0
            at = PART * k + SLOT * half
            w_ref[at : at + SLOT, :] = jnp.where(row < UNITS, w[0:SLOT], fill).astype(BF16)
    r = iota((128, COLS), 0)
    ratio = gb_buf[1] / gain
    rh = rounded(ratio)
    lead = jnp.where(r == 0, 1.0, jnp.where(r == 1, rh, jnp.where(r == 2, ratio - rh, 0.0))).astype(BF16)
    cols = dot(w_ref[...], lead, 1, 1)
    col = cols[:, 0:1]
    sums = cols.T
    both = jnp.concatenate([sums[0:1], sums[1:2] + sums[2:3], jnp.zeros((1, ROWS - 8 * PART), F32)], axis=1)
    hi = rounded(both)
    q = iota((8, ROWS), 0)
    vec_ref[...] = jnp.where(q == 0, hi, jnp.where(q == 1, both - hi, 0.0))

    stores = []
    for j in range(4 // PER):
        at = slice(TILE * j, TILE * (j + 1))
        for copy in tokens[9 * PER * j : 9 * PER * (j + 1)]:
            copy.wait()
        part = dot(w_ref[...], x_buf[PER * j : PER * (j + 1)].reshape(TILE, COLS), 1, 1)
        x = x_buf[PER * j : PER * (j + 1)].reshape(TILE, COLS).astype(F32)
        pivot = x[:, 0:1]
        c = x - pivot
        sq = jnp.sum(c * c, axis=1, keepdims=True)
        lane = iota((TILE, 128), 1)
        stat = jnp.where(lane == 0, sq, jnp.where(lane == 1, pivot, 0.0)).T
        m_row = part[UNITS : UNITS + 1] * (1.0 / COLS)
        off = m_row - stat[1:2]
        m2_row = stat[0:1] - COLS * off * off
        m_hi = rounded(m_row)
        m_mid = rounded(m_row - m_hi)
        m_lo = m_row - m_hi - m_mid
        m2_hi = rounded(m2_row)
        m2_lo = m2_row - m2_hi
        r = iota((8, TILE), 0)
        t1 = jnp.where(r == 4, m_hi, jnp.where(r == 5, m_mid, jnp.where(r == 6, m_lo, jnp.where(r == 7, vec_ref[0:1, at], 0.0))))
        t2 = jnp.where(r == 4, m2_hi, jnp.where(r == 5, m2_lo, jnp.where(r == 6, vec_ref[1:2, at], 0.0)))
        z = jnp.zeros((SLOT - 8, TILE), F32)
        extra = jnp.concatenate([z, t1, z, t2], axis=0)
        for k in range(4):
            rows = slice(PART * k, PART * (k + 1))
            out_buf[k, :, at] = (part[rows] - col[rows] * m_row + extra).astype(BF16)
        stores.append(pltpu.make_async_copy(out_buf.at[:, :, at], out_ref.at[:, :, at], sems.at[40 + j]))
        stores[-1].start()
    for copy in stores:
        copy.wait()


def project(tokens, gate_t, up_t, gain, bias):
    hbm = pl.BlockSpec(memory_space=pl.ANY)
    return pl.pallas_call(
        project_kernel,
        in_specs=[hbm] * 5,
        out_specs=hbm,
        out_shape=pltpu.HBM((4, PART, ROWS), BF16),
        scratch_shapes=[
            pltpu.VMEM((4, 4, 4, 16, COLS), BF16),
            pltpu.VMEM((FFL, COLS), F32),
            pltpu.VMEM((FFL, COLS), F32),
            pltpu.VMEM((2, 1, COLS), F32),
            pltpu.VMEM((4, PART, ROWS), BF16),
            pltpu.VMEM((4 * PART, COLS), BF16),
            pltpu.VMEM((8, ROWS), F32),
            pltpu.SemaphoreType.DMA((44,)),
        ],
        name="project",
    )(*[pltpu.with_memory_space_constraint(a, pltpu.HBM) for a in (tokens.reshape(4, 2, 4, 2, 16, COLS), gate_t, up_t, gain, bias)])


def hidden_kernel(r_ref, gs_ref, us_ref, out_ref, stat_ref):
    me = lax.axis_index("cb")
    means = []
    m2s = []
    for c in range(4):
        a = r_ref[c, 32:48, :].astype(F32)
        b = r_ref[c, 80:96, :].astype(F32)
        means.append(a[12:13] + a[13:14] + a[14:15])
        m2s.append(b[12:13] + b[13:14])
    mean = (means[0] + means[1] + means[2] + means[3]) * 0.25
    deltas = [v - mean for v in means]
    m2 = sum(m2s) + COLS * sum(d * d for d in deltas)
    rstd = lax.rsqrt(m2 * (1.0 / D) + 1e-05)
    q = iota((8, ROWS), 0)
    stat_ref[...] = jnp.where(q == 0, mean, jnp.where(q == 1, rstd, 0.0))

    wide = 8 * PART
    pick_row = iota((2 * PART, wide), 0)
    pick_lane = iota((2 * PART, wide), 1)
    base = jnp.where(pick_row < PART, me * PART, (4 + me) * PART - PART)
    pick = one_hot(pick_lane == pick_row + base)
    tiles = [r_ref[c, 32:48, 0:wide] for c in range(4)] + [r_ref[c, 80:96, 0:wide] for c in range(4)]
    vecs = dot(pick, jnp.concatenate(tiles, axis=0), 1, 1)
    col_sums = [vecs[0:PART, 16 * c + 15 : 16 * c + 16] + vecs[0:PART, 78 + 16 * c : 79 + 16 * c] for c in range(4)]
    biases = sum(vecs[PART:, 16 * c + 15 : 16 * c + 16] + vecs[PART:, 78 + 16 * c : 79 + 16 * c] for c in range(4))

    gs = gs_ref[...]
    us = us_ref[...]
    g1 = rounded(gs)
    g2 = rounded(gs - g1)
    u1 = rounded(us)
    u2 = rounded(us - u1)
    sr = iota((16, FFL), 0)
    pieces = jnp.where(sr == 0, g1, jnp.where(sr == 1, g2, jnp.where(sr == 2, gs - g1 - g2, 0.0)))
    pieces = pieces + jnp.where(sr == 3, u1, jnp.where(sr == 4, u2, jnp.where(sr == 5, us - u1 - u2, 0.0)))
    row = iota((PART, FFL), 0)
    unit = jnp.where(row < SLOT, row, row - SLOT)
    own = one_hot((iota((PART, FFL), 1) == unit + me * UNITS) & (unit < UNITS))
    sc = dot(own, pieces.astype(BF16), 1, 1)
    scale = jnp.where(iota((PART, 1), 0) < SLOT, sc[:, 0:1] + sc[:, 1:2] + sc[:, 2:3], sc[:, 3:4] + sc[:, 4:5] + sc[:, 5:6])

    keep = iota((SLOT, CHUNK), 0) < UNITS
    turn = 2 * flipped(lax.axis_index("Z")) + flipped(lax.axis_index("Y"))
    for j in range(4):
        at = slice(CHUNK * j, CHUNK * (j + 1))
        acc = jnp.zeros((PART, CHUNK), F32)
        for c in range(4):
            acc = acc + (r_ref[c, :, at].astype(F32) + col_sums[c] * deltas[c][:, at])
        y = (acc * rstd[:, at] + biases) * scale
        gate = y[0:SLOT]
        up = y[SLOT:PART]
        h = jnp.where(keep, gate / (1.0 + jnp.exp(-gate)) * up, 0.0).astype(BF16)
        for k in range(4):
            out_ref[k, j ^ turn] = h


def hidden_of(received, gate_scale, up_scale):
    vm = pl.BlockSpec(memory_space=pltpu.VMEM)
    return pl.pallas_call(
        hidden_kernel,
        in_specs=[vm, vm, vm],
        out_specs=[vm, vm],
        out_shape=[pltpu.VMEM((4, 4, SLOT, CHUNK), BF16), pltpu.VMEM((8, ROWS), F32)],
        name="hidden",
    )(*[near(a) for a in (received, gate_scale, up_scale)])


def down_kernel(h_ref, own_ref, fetched_ref, other_ref, out_ref):
    me = lax.axis_index("zl") * 2 + lax.axis_index("yl")
    core = lax.axis_index("dp")

    unit = iota((FFL, 4 * SLOT), 0)
    slot = jnp.where(unit < 2 * UNITS, jnp.where(unit < UNITS, 0, 1), jnp.where(unit < 3 * UNITS, 2, 3))
    place = one_hot(iota((FFL, 4 * SLOT), 1) == unit + (SLOT - UNITS) * slot)

    def squeezed(member):
        h = jnp.concatenate([h_ref[k, member] for k in range(4)], axis=0)
        return dot(h, place, 0, 1).astype(BF16)

    acc = dot(squeezed(me), own_ref[...], 1, 0)
    acc = acc + dot(squeezed(me ^ (1 + core)), fetched_ref[:, 0:COLS], 1, 0)
    acc = acc + dot(squeezed(me ^ (2 - core)), other_ref[:, 0:COLS], 1, 0)
    h = squeezed(me ^ 3)
    mine = dot(h, fetched_ref[:, COLS:], 1, 0)
    theirs = dot(h, other_ref[:, COLS:], 1, 0)
    acc = acc + jnp.concatenate([jnp.where(core == 0, mine, theirs), jnp.where(core == 0, theirs, mine)], axis=1)
    out_ref[...] = acc.astype(BF16)


def down(hidden, weights):
    vm = pl.BlockSpec(memory_space=pltpu.VMEM)
    return pl.pallas_call(
        down_kernel,
        in_specs=[vm] * 4,
        out_specs=vm,
        out_shape=pltpu.VMEM((CHUNK, COLS), BF16),
        name="down",
    )(near(hidden), *[near(w) for w in weights])


def mix_kernel(r_ref, x_ref, stat_ref, gain_ref, bias_ref, scale_ref, mixed_ref, part_ref):
    member = (lax.axis_index("zl") ^ flipped(lax.axis_index("Z"))) * 2 + (lax.axis_index("yl") ^ flipped(lax.axis_index("Y")))
    at = member * CHUNK + (lax.axis_index("Z") * 4 + lax.axis_index("Y")) * 16
    branch = jnp.zeros((16, COLS), F32)
    for k in range(16):
        branch = branch + r_ref[k].astype(F32)
    mine = iota((16, ROWS), 1) == iota((16, ROWS), 0) + at
    mean = jnp.sum(jnp.where(mine, stat_ref[0:1], 0.0), axis=1, keepdims=True)
    rstd = jnp.sum(jnp.where(mine, stat_ref[1:2], 0.0), axis=1, keepdims=True)
    normed = rounded((x_ref[...].astype(F32) - mean) * rstd * gain_ref[...] + bias_ref[...])
    mixed = 0.5 * normed + branch * scale_ref[...]
    mixed_ref[...] = mixed
    m = jnp.sum(mixed, axis=1, keepdims=True) * (1.0 / COLS)
    c = mixed - m
    m2 = jnp.sum(c * c, axis=1, keepdims=True)
    lane = iota((16, 128), 1)
    part = jnp.where(lane == 0, m, jnp.where(lane == 1, m2, 0.0))
    for k in range(4):
        part_ref[k] = part


def mix(received, own, stats, gain, bias, scale):
    vm = pl.BlockSpec(memory_space=pltpu.VMEM)
    return pl.pallas_call(
        mix_kernel,
        in_specs=[vm] * 6,
        out_specs=[vm, vm],
        out_shape=[pltpu.VMEM((16, COLS), F32), pltpu.VMEM((4, 16, 128), F32)],
        name="mix",
    )(*[near(a) for a in (received, own, stats, gain, bias, scale)])


def finish_kernel(mixed_ref, part_ref, gain_ref, bias_ref, out_ref):
    parts = [part_ref[k] for k in range(4)]
    means = [p[:, 0:1] for p in parts]
    mean = (means[0] + means[1] + means[2] + means[3]) * 0.25
    m2 = sum(p[:, 1:2] for p in parts) + COLS * sum((v - mean) * (v - mean) for v in means)
    rstd = lax.rsqrt(m2 * (1.0 / D) + 1e-05)
    out_ref[...] = ((mixed_ref[...] - mean) * rstd * gain_ref[...] + bias_ref[...]).astype(BF16)


def finish(mixed, parts, gain, bias):
    vm = pl.BlockSpec(memory_space=pltpu.VMEM)
    return pl.pallas_call(
        finish_kernel,
        in_specs=[vm] * 4,
        out_specs=vm,
        out_shape=jax.ShapeDtypeStruct((16, COLS), BF16),
        name="finish",
    )(*[near(a) for a in (mixed, parts, gain, bias)])


def flipped(z):
    return (z ^ (z >> 1)) & 1


def spread_groups():
    return [
        [(2 * z + (jz ^ flipped(z))) * 8 + 2 * y + (jy ^ flipped(y)) for z in range(4) for y in range(4)]
        for jz in range(2)
        for jy in range(2)
    ]


def swapped(n, k):
    return [(i, i ^ k) for i in range(n)]


def local(
    tokens,
    norm_gain,
    norm_bias,
    gate_weight,
    up_weight,
    gate_scale,
    up_scale,
    down_weight,
    down_scale,
    out_gain,
    out_bias,
):
    gain = norm_gain.reshape(1, COLS)
    bias = norm_bias.reshape(1, COLS)

    w0 = down_weight.astype(BF16)
    beside = lax.ppermute(w0, ("zl", "yl", "dp"), [(i, i ^ (4 if i & 1 else 2)) for i in range(8)])
    half = lax.dynamic_slice_in_dim(w0, lax.axis_index("dp") * (COLS // 2), COLS // 2, 1)
    across = lax.ppermute(half, ("zl", "yl"), swapped(4, 3))

    shares = project(tokens, gate_weight.T, up_weight.T, gain, bias)
    received = lax.all_to_all(shares, "cb", 0, 0, tiled=True)
    sent, stats = hidden_of(received, gate_scale.reshape(1, FFL), up_scale.reshape(1, FFL))
    own = lax.dynamic_slice_in_dim(tokens, lax.axis_index(RA) * 16, 16, 0)
    sent, own = lax.optimization_barrier((sent, own))
    hidden = lax.all_to_all(sent.reshape(16, SLOT, CHUNK), ("cb", "zl", "yl"), 0, 0, tiled=True)
    fetched = jnp.concatenate([beside, across], axis=1)
    other = lax.ppermute(fetched, "dp", swapped(2, 1))
    partial = down(hidden.reshape(4, 4, SLOT, CHUNK), (w0, fetched, other))
    pieces = lax.all_to_all(
        partial.reshape(16, 16, COLS), RA, 0, 0, axis_index_groups=spread_groups(), tiled=True
    )
    mixed, part = mix(pieces, own, stats, gain, bias, down_scale.reshape(1, COLS))
    parts = lax.all_to_all(part, "cb", 0, 0, tiled=True)
    return finish(mixed, parts, out_gain.reshape(1, COLS), out_bias.reshape(1, COLS))


def solution(mesh):
    split = Mesh(mesh.devices.reshape(4, 2, 4, 2, 4, 2), RA + ("cb", "dp"))
    return jax.shard_map(
        local,
        mesh=split,
        in_specs=(
            P("dp", "cb"),
            P("cb"),
            P("cb"),
            P("cb", RA),
            P("cb", RA),
            P(RA),
            P(RA),
            P(RA, "cb"),
            P("cb"),
            P("cb"),
            P("cb"),
        ),
        out_specs=P(("dp",) + RA, "cb"),
        check_vma=False,
    )
```
